32 devices in a mesh: kv: 8 (over z, y), tp: 4 (over x, core).
Axes of the slice: x: 2, y: 2, z: 4, core: 2. Of those that a mesh axis runs over, the one named last changes fastest.
Arguments:
- tokens: bfloat16 [64, 4096], P(None, 'kv'), may hold values from -8 to 8
- attn_gain: float32 [4096], P('kv'), may hold values from 0.1 to 1.9
- w_query: bfloat16 [4096, 2048], P('kv', 'tp'), may hold values from -0.09375 to 0.09375
- w_key: bfloat16 [4096, 2048], P('kv', 'tp'), may hold values from -0.09375 to 0.09375
- w_value: bfloat16 [4096, 4096], P('kv', 'tp'), may hold values from -0.09375 to 0.09375
- w_outgate: bfloat16 [4096, 4096], P('kv', 'tp'), may hold values from -0.09375 to 0.09375
- w_gates: bfloat16 [4096, 16], replicated, may hold values from -0.029907227 to 0.029907227
- forget_bias: float32 [8], replicated, may hold values from -1 to 3
- state_c: float32 [64, 8, 512, 256], P('kv', 'tp'), may hold values from -6 to 6
- state_n: float32 [64, 8, 256], P('kv', 'tp'), may hold values from -6 to 6
- state_m: float32 [64, 8], P('kv', 'tp'), may hold values from -2 to 0.5
- w_output: bfloat16 [4096, 4096], P('tp', 'kv'), may hold values from -0.09375 to 0.09375
- mlp_gain: float32 [4096], P('kv'), may hold values from 0.1 to 1.9
- w_gateff: bfloat16 [4096, 11008], P('kv', 'tp'), may hold values from -0.09375 to 0.09375
- w_upff: bfloat16 [4096, 11008], P('kv', 'tp'), may hold values from -0.09375 to 0.09375
- w_downff: bfloat16 [11008, 4096], P('tp', 'kv'), may hold values from -0.0546875 to 0.0546875
Outputs:
- mixed: bfloat16 [64, 4096], P(None, 'kv')
- new_c: float32 [64, 8, 512, 256], P('kv', 'tp')
- new_n: float32 [64, 8, 256], P('kv', 'tp')
- new_m: float32 [64, 8], P('kv', 'tp')
The draws below stay inside these ranges and needn't reach their ends.
All inputs are finite; a program needn't handle non-finite values.
Results may differ from the reference program's by a relative error of at most 0.0083.
Values may be sent and summed in bfloat16 or wider, within the bound.
A program may use at most 64 MiB of HBM per device.

```python
import math
import jax
import jax.numpy as jnp
from jax import lax

D = 4096
HEADS = 8
DQK = 256
DV = 512
FF = 11008
BATCH = 64


def draw_tokens(key, part):
    key_scale = jax.random.fold_in(key, 11)
    key_values = jax.random.fold_in(key, 12)
    groups = D // 16
    scales = jnp.exp(jax.random.uniform(key_scale, (groups,), jnp.float32, math.log(0.3), math.log(3.0)))
    scales = jnp.repeat(scales, 16)
    values = jax.random.normal(key_values, (BATCH, D), jnp.float32)
    return jnp.clip(values * scales[None, :], -8.0, 8.0).astype(jnp.bfloat16)


def level_of(rng, extent, shards, smallest, largest):
    def one(position, blocks):
        heights = jax.random.uniform(jax.random.fold_in(jax.random.fold_in(rng, 6), position), (blocks,), jnp.float32, smallest / len(shards), largest / len(shards))
        return jnp.repeat(jnp.exp(heights), extent[position] // blocks).reshape((-1,) + (1,) * (len(extent) - position - 1))

    loudness = one(*shards[0])
    for cut in shards[1:]:
        loudness = loudness * one(*cut)
    return loudness


def normal_values(stream_key, extent, deviation, limit, pieces=(), held_as=jnp.bfloat16):
    entries = jax.random.normal(stream_key, extent, jnp.float32) * deviation
    if len(pieces) > 0:
        entries = level_of(stream_key, extent, pieces, -0.22, 0.18) * entries
    return jnp.clip(entries, min=-limit, max=limit).astype(held_as)


def setup_inputs(seed: int = 0) -> dict:
    streams_of = jax.random.split(jax.random.key(seed), 17)
    return {
        "tokens": draw_tokens(jax.random.fold_in(streams_of[16], 71), 0),
        "attn_gain": jnp.clip(1.0 + 0.18 * jax.random.normal(streams_of[1], (D,), jnp.float32), 0.1, 1.9),
        "w_query": normal_values(streams_of[2], (D, HEADS * DQK), D ** -0.5, 0.09375, ((0, 8), (1, 4))),
        "w_key": normal_values(streams_of[3], (D, HEADS * DQK), D ** -0.5, 0.09375, ((0, 8), (1, 4))),
        "w_value": normal_values(streams_of[4], (D, HEADS * DV), D ** -0.5, 0.09375, ((0, 8), (1, 4))),
        "w_outgate": normal_values(streams_of[5], (D, HEADS * DV), D ** -0.5, 0.09375, ((0, 8), (1, 4))),
        "w_gates": normal_values(streams_of[6], (D, 2 * HEADS), 0.0047, 0.029907227),
        "forget_bias": jnp.clip(jax.random.uniform(streams_of[7], (HEADS,), jnp.float32, -1.0, 3.0), -1.0, 3.0),
        "state_c": normal_values(streams_of[8], (BATCH, HEADS, DV, DQK), 1.0, 6.0, ((0, 8), (1, 4)), jnp.float32),
        "state_n": normal_values(streams_of[9], (BATCH, HEADS, DQK), 1.0, 6.0, ((0, 8), (1, 4)), jnp.float32),
        "state_m": jnp.clip(-2.0 + 2.5 * jax.random.uniform(streams_of[10], (BATCH, HEADS), jnp.float32) ** level_of(streams_of[10], (BATCH, HEADS), ((0, 8), (1, 4)), -0.2, 0.2), -2.0, 0.5),
        "w_output": normal_values(streams_of[11], (HEADS * DV, D), (HEADS * DV) ** -0.5, 0.09375, ((0, 4), (1, 8))),
        "mlp_gain": jnp.clip(1.0 + 0.18 * jax.random.normal(streams_of[12], (D,), jnp.float32), 0.1, 1.9),
        "w_gateff": normal_values(streams_of[13], (D, FF), D ** -0.5, 0.09375, ((0, 8), (1, 4))),
        "w_upff": normal_values(streams_of[14], (D, FF), D ** -0.5, 0.09375, ((0, 8), (1, 4))),
        "w_downff": normal_values(streams_of[15], (FF, D), FF ** -0.5, 0.0546875, ((0, 4), (1, 8))),
    }


norm_floor = 1e-05

def inverse_rms(values):
    return lax.rsqrt(lax.optimization_barrier(jnp.mean(values * values, axis=-1)) + norm_floor)

def reference(tokens, attn_gain, w_query, w_key, w_value, w_outgate, w_gates, forget_bias, state_c, state_n, state_m, w_output, mlp_gain, w_gateff, w_upff, w_downff):
    batch = tokens.shape[0]
    tok_float = tokens.astype(jnp.float32)
    scale_one = inverse_rms(tok_float)[:, None]
    normed_one = (tok_float * attn_gain).astype(jnp.bfloat16)

    def project(weight):
        return jnp.dot(normed_one, weight, preferred_element_type=jnp.float32) * scale_one
    query = (project(w_query) * DQK ** (-0.5)).reshape(batch, HEADS, DQK)
    key_vec = project(w_key).reshape(batch, HEADS, DQK)
    value = project(w_value).reshape(batch, HEADS, DV)
    out_pre = project(w_outgate).reshape(batch, HEADS, DV)
    gate_pre = project(w_gates)
    log_input = gate_pre[:, :HEADS]
    log_forget = jax.nn.log_sigmoid(gate_pre[:, HEADS:] + forget_bias)
    carried = log_forget + state_m
    new_m = jnp.maximum(carried, log_input)
    keep = jnp.exp(carried - new_m)
    admit = jnp.exp(log_input - new_m)
    new_c = keep[:, :, None, None] * state_c + admit[:, :, None, None] * value[:, :, :, None] * key_vec[:, :, None, :]
    new_n = keep[:, :, None] * state_n + admit[:, :, None] * key_vec
    numer = jnp.einsum('bhvd,bhd->bhv', new_c, query, precision=lax.Precision.HIGHEST)
    denom = jnp.maximum(jnp.abs(lax.optimization_barrier(jnp.sum(new_n * query, axis=-1))), jnp.exp(-new_m))
    head_out = (jax.nn.sigmoid(out_pre) * numer / denom[:, :, None]).reshape(batch, HEADS * DV).astype(jnp.bfloat16)
    attn_mix = jnp.dot(head_out, w_output, preferred_element_type=jnp.float32)
    middle = (tok_float + attn_mix).astype(jnp.bfloat16)
    mid_float = middle.astype(jnp.float32)
    scale_two = inverse_rms(mid_float)[:, None]
    normed_two = (mid_float * mlp_gain).astype(jnp.bfloat16)
    gate_ff = jnp.dot(normed_two, w_gateff, preferred_element_type=jnp.float32) * scale_two
    up_ff = jnp.dot(normed_two, w_upff, preferred_element_type=jnp.float32) * scale_two
    hidden_ff = (jax.nn.silu(gate_ff) * up_ff).astype(jnp.bfloat16)
    mixed = (mid_float + jnp.dot(hidden_ff, w_downff, preferred_element_type=jnp.float32)).astype(jnp.bfloat16)
    return (mixed, new_c, new_n, new_m)
```

```python
import jax
import jax.numpy as jnp
from jax import lax
from jax.experimental import pallas as pl
from jax.experimental.pallas import tpu as pltpu
from jax.sharding import PartitionSpec as P

norm_floor = 1e-05
MESH = pl.DeviceIdType.MESH
LANES = 128
SPAN = 512
VMEM_ALL = 67043328
ROOM = 4 * 1024 * 1024
VMEM_SPEC = pl.BlockSpec(memory_space=pltpu.VMEM)
HBM_SPEC = pl.BlockSpec(memory_space=pltpu.HBM)
F32, BF16 = jnp.float32, jnp.bfloat16


def peer_of(axis, step):
    count = lax.axis_size(axis)
    return lax.rem(lax.axis_index(axis) + step, count)


def signal_peers(barrier, axis):
    for step in range(1, lax.axis_size(axis)):
        pl.semaphore_signal(
            barrier, inc=1, device_id={axis: peer_of(axis, step)}, device_id_type=MESH
        )


def inner_size(count):
    size = 1 << ((count.bit_length() - 1) // 2)
    return size if count % size == 0 else 1


def place():
    count = lax.axis_size("kv")
    inner = inner_size(count)
    kv = lax.axis_index("kv")
    return kv // inner, kv % inner, count // inner, inner


def inner_peer(step):
    outer_at, inner_at, _, inner = place()
    return (inner_at + step) % inner, outer_at * inner + (inner_at + step) % inner


def outer_peer(step):
    outer_at, inner_at, outer, inner = place()
    return (outer_at + step) % outer, ((outer_at + step) % outer) * inner + inner_at


def send_to(axis, device, src, dst, send_sem, recv_sem):
    copy = pltpu.make_async_remote_copy(
        src_ref=src,
        dst_ref=dst,
        send_sem=send_sem,
        recv_sem=recv_sem,
        device_id={axis: device},
        device_id_type=MESH,
    )
    copy.start()
    return copy


def put_part(part, out, at, size):
    inner, outer, rows, _ = part.shape
    split = out.reshape(outer, inner, rows, size).astype(part.dtype)
    for i in range(inner):
        part[i, :, :, at : at + size] = split[:, i]


class Scatter:
    def __init__(self, part, land, both, last, esend, erecv, fsend, frecv):
        self.part, self.land, self.both, self.last = part, land, both, last
        self.esend, self.erecv, self.fsend, self.frecv = esend, erecv, fsend, frecv
        self.gone = []

    def first(self):
        inner = self.part.shape[0]
        self.one = []
        for step in range(1, inner):
            at, device = inner_peer(step)
            self.one.append(
                send_to(
                    "kv", device, self.part.at[at], self.land.at[step],
                    self.esend.at[step], self.erecv.at[step],
                )
            )
        self.gone += self.one

    def second(self):
        _, inner_at, outer, inner = place()
        for copy in self.one:
            copy.wait_recv()
        acc = self.part[inner_at].astype(F32)
        for step in range(1, inner):
            acc += self.land[step].astype(F32)
        self.both[...] = acc.astype(self.both.dtype)
        self.two = []
        for step in range(1, outer):
            to, device = outer_peer(step)
            self.two.append(
                send_to(
                    "kv", device, self.both.at[to], self.last.at[step],
                    self.fsend.at[step], self.frecv.at[step],
                )
            )
        self.gone += self.two

    def total(self):
        outer_at, _, outer, _ = place()
        for copy in self.two:
            copy.wait_recv()
        acc = self.both[outer_at].astype(F32)
        for step in range(1, outer):
            acc += self.last[step].astype(F32)
        return acc


def scatter_scratch(inner, outer, rows, wide, dtype):
    sem = pltpu.SemaphoreType.DMA
    return [
        pltpu.VMEM((inner, outer, rows, wide), dtype),
        pltpu.VMEM((inner, outer, rows, wide), dtype),
        pltpu.VMEM((outer, rows, wide), dtype),
        pltpu.VMEM((outer, rows, wide), dtype),
        sem((inner,)),
        sem((inner,)),
        sem((outer,)),
        sem((outer,)),
    ]


class Gather:
    def __init__(self, buf, asend, arecv, bsend, brecv):
        self.buf = buf
        self.asend, self.arecv, self.bsend, self.brecv = asend, arecv, bsend, brecv
        self.gone = []

    def send(self):
        outer_at, inner_at, outer, inner = place()
        own = self.buf.at[outer_at, inner_at]
        self.along = []
        self.across = []
        for step in range(1, outer):
            self.along.append(
                send_to("kv", outer_peer(step)[1], own, own, self.asend.at[step], self.arecv.at[step])
            )
        self._across(0)
        self.gone += self.along

    def _across(self, far):
        outer_at, inner_at, outer, inner = place()
        block = self.buf.at[(outer_at + outer - far) % outer, inner_at]
        for step in range(1, inner):
            copy = send_to(
                "kv", inner_peer(step)[1], block, block, self.bsend.at[far, step], self.brecv.at[far, step]
            )
            self.across.append(copy)
            self.gone.append(copy)

    def relay(self):
        for far, copy in enumerate(self.along):
            copy.wait_recv()
            self._across(far + 1)

    def wait(self):
        for copy in self.across:
            copy.wait_recv()


def gather_scratch(inner, outer, rows, wide):
    sem = pltpu.SemaphoreType.DMA
    return [
        pltpu.VMEM((outer, inner, rows, wide), BF16),
        sem((outer,)),
        sem((outer,)),
        sem((outer, inner)),
        sem((outer, inner)),
    ]


def tp_total(buf, send_sem, recv_sem):
    tp = lax.axis_index("tp")
    count = lax.axis_size("tp")
    copies = [
        send_to("tp", peer_of("tp", step), buf.at[tp], buf.at[tp], send_sem.at[step], recv_sem.at[step])
        for step in range(1, count)
    ]
    for copy in copies:
        copy.wait_recv()
    total = buf[0].astype(F32)
    for i in range(1, count):
        total += buf[i].astype(F32)
    return total, copies


def padded(wide):
    return -(-wide // LANES) * LANES


def hidden_spans(hidden):
    return [(at, min(SPAN, hidden - at)) for at in range(0, hidden, SPAN)]


def ffn_order(spans):
    events = []
    for k in range(spans):
        events += [(3.4 + 1.25 * k, 0, k), (7.8 + 1.25 * k, 1, k), (12.0 + 1.25 * k, 2, k), (14.5 + 1.25 * k, 3, k)]
    return [(kind, k) for _, kind, k in sorted(events)]


def layer_kernel(heads, spans, *refs):
    (
        tok_hbm, gain1_hbm, wq, wk, wv, wo, wg, bias_hbm, m_hbm, n_hbm, c_hbm, wout, gain2_hbm, wgf, wuf, wdf,
        mixed_ref, newc_ref, newn_ref, newm_ref,
    ) = refs[:20]
    scratch = list(refs[20:])

    def take(n):
        got = scratch[:n]
        del scratch[:n]
        return got

    tok_v, gain1_v, wq_v, wk_v, wv_v, wo_v, wg_v, wout_v, wgf_v, wuf_v, wdf_v = take(11)
    bias_ref, m_ref, n_ref, gain2_ref = take(4)
    wload, cload, sload = take(3)
    gates_rs = Scatter(*take(8))
    proj_rs = [Scatter(*take(8)) for _ in range(2 + 2 * heads)]
    head_ag = [Gather(*take(5)) for _ in range(heads)]
    ffn_rs = [Scatter(*take(8)) for _ in spans]
    square_rs = Scatter(*take(8))
    ffn_ag = [Gather(*take(5)) for _ in spans]
    abuf, dbuf, mid_v, acc_v, cols_v, asend, arecv, dsend, drecv = take(9)

    kv = lax.axis_index("kv")
    tp = lax.axis_index("tp")
    count = lax.axis_size("kv")
    outer_at, inner_at, outer, inner = place()
    batch, width = tok_v.shape
    rows = batch // count
    _, _, value_size, query_size = newc_ref.shape
    heads_all = bias_ref.shape[1]
    gate_cols = wg_v.shape[0]

    barrier = pltpu.get_barrier_semaphore()
    signal_peers(barrier, "kv")
    signal_peers(barrier, "tp")
    chunks = [(wq, wq_v, 0, heads * query_size), (wk, wk_v, 0, heads * query_size)]
    for h in range(heads):
        chunks.append((wv, wv_v, h * value_size, value_size))
        chunks.append((wo, wo_v, h * value_size, value_size))
    early = [
        pltpu.make_async_copy(tok_hbm, tok_v, wload.at[0]),
        pltpu.make_async_copy(gain1_hbm, gain1_v, wload.at[1]),
        pltpu.make_async_copy(
            wg.at[:, pl.ds(pl.multiple_of(kv * width, LANES), width)], wg_v, wload.at[2]
        ),
    ]
    for load in early:
        load.start()
    small = [
        pltpu.make_async_copy(src, dst, sload.at[i])
        for i, (src, dst) in enumerate(
            [(bias_hbm, bias_ref), (m_hbm, m_ref), (n_hbm, n_ref), (gain2_hbm, gain2_ref)]
        )
    ]
    for load in small:
        load.start()
    loads = []
    for i, (src, dst, at, wide) in enumerate(chunks):
        load = pltpu.make_async_copy(
            src.at[:, pl.ds(at, wide)], dst.at[:, pl.ds(at, wide)], wload.at[7 + i]
        )
        load.start()
        loads.append(load)
    early[0].wait()
    early[1].wait()
    tok = tok_v[...].astype(F32)
    squares = jnp.sum(tok * tok, axis=1, keepdims=True)
    normed = (tok * gain1_v[...]).astype(BF16)
    ready = []
    for i, (_, dst, at, wide) in enumerate(chunks):
        loads[i].wait()
        out = jnp.dot(normed, dst[:, at : at + wide], preferred_element_type=F32)
        put_part(proj_rs[i].part, out, 0, wide)
        if i == 1:
            early[2].wait()
            gates = lax.dot_general(
                normed, wg_v[...], (((1,), (1,)), ((), ())), preferred_element_type=F32
            )
            put_part(gates_rs.part, jnp.broadcast_to(squares, (batch, LANES)), 0, LANES)
            put_part(gates_rs.part, gates, 0, gate_cols)
            pl.semaphore_wait(barrier, count - 1 + lax.axis_size("tp") - 1)
            proj_rs[0].first()
            gates_rs.first()
            proj_rs[1].first()
        elif i > 1:
            proj_rs[i].first()
    cloads = [
        [pltpu.make_async_copy(c_hbm.at[b, h], newc_ref.at[b, h], cload.at[b, h]) for b in range(rows)]
        for h in range(heads)
    ]
    for group in cloads:
        for load in group:
            load.start()
    late = [
        pltpu.make_async_copy(src, dst, wload.at[3 + i])
        for i, (src, dst) in enumerate([(wout, wout_v), (wgf, wgf_v), (wuf, wuf_v), (wdf, wdf_v)])
    ]
    for load in late:
        load.start()
    for load in small:
        load.wait()
    proj_rs[0].second()
    gates_rs.second()
    for rs in proj_rs[1:]:
        rs.second()

    scale_query = proj_rs[0].total()
    gate_sum = gates_rs.total()
    scale = lax.rsqrt(gate_sum[:, gate_cols : gate_cols + 1] / (width * count) + norm_floor)
    gates = gate_sum * scale
    query_all = scale_query * (scale * query_size ** (-0.5))
    query_low = query_all.astype(BF16)
    lane = lax.broadcasted_iota(jnp.int32, gates.shape, 1)
    bias_lane = lax.broadcasted_iota(jnp.int32, bias_ref.shape, 1)
    sub = lax.broadcasted_iota(jnp.int32, (rows, value_size), 0)
    eye = lax.broadcasted_iota(jnp.int32, (rows, rows), 0) == lax.broadcasted_iota(
        jnp.int32, (rows, rows), 1
    )
    keeps, admits, new_ms = [], [], []
    for h in range(heads):
        column = tp * heads + h
        log_input = jnp.sum(jnp.where(lane == column, gates, 0.0), axis=1, keepdims=True)
        forget = jnp.sum(jnp.where(lane == heads_all + column, gates, 0.0), axis=1, keepdims=True)
        bias = jnp.sum(jnp.where(bias_lane == column, bias_ref[...], 0.0), axis=1, keepdims=True)
        pre = forget + bias
        log_forget = jnp.minimum(pre, 0.0) - jnp.log(1.0 + jnp.exp(-jnp.abs(pre)))
        old_m = jnp.sum(jnp.where(eye, m_ref[h : h + 1, :], 0.0), axis=1, keepdims=True)
        carried = log_forget + old_m
        new_m = jnp.maximum(carried, log_input)
        keeps.append(jnp.exp(carried - new_m))
        admits.append(jnp.exp(log_input - new_m))
        new_ms.append(new_m)
        newm_ref[h : h + 1, :] = jnp.sum(jnp.where(eye, new_m, 0.0), axis=0, keepdims=True)
    reads = []
    for h in range(heads):
        read = jnp.zeros((rows, value_size), F32)
        low = query_low[:, h * query_size : (h + 1) * query_size]
        for b in range(rows):
            cloads[h][b].wait()
            one = lax.dot_general(
                low, newc_ref[b, h].astype(BF16), (((1,), (1,)), ((), ())), preferred_element_type=F32
            )
            read = jnp.where(sub == b, one, read)
        reads.append(read)
    key_all = proj_rs[1].total() * scale
    keys = []
    for h in range(heads):
        query = query_all[:, h * query_size : (h + 1) * query_size]
        key = admits[h] * key_all[:, h * query_size : (h + 1) * query_size]
        keys.append(key)
        new_n = keeps[h] * n_ref[:, h, :] + key
        newn_ref[:, h, :] = new_n
        denom = jnp.maximum(
            jnp.abs(jnp.sum(new_n * query, axis=1, keepdims=True)), jnp.exp(-new_ms[h])
        )
        value = proj_rs[2 + 2 * h].total() * scale
        numer = keeps[h] * reads[h] + value * jnp.sum(key * query, axis=1, keepdims=True)
        cols_v[h] = value.T
        out_pre = proj_rs[3 + 2 * h].total() * scale
        gated = numer / ((1.0 + jnp.exp(-out_pre)) * denom)
        head_ag[h].buf[outer_at, inner_at] = gated.astype(BF16)
        head_ag[h].send()
    for h in range(heads):
        keep_wide = jnp.broadcast_to(keeps[h], (rows, query_size))
        for b in range(rows):
            newc_ref[b, h] = (
                keep_wide[b : b + 1, :] * newc_ref[b, h] + cols_v[h, :, b : b + 1] * keys[h][b : b + 1, :]
            )
        if h == 0:
            for ag in head_ag:
                ag.relay()

    late[0].wait()
    attn = None
    for h in range(heads):
        head_ag[h].wait()
        block = head_ag[h].buf[...].astype(F32).reshape(batch, value_size).astype(BF16)
        one = jnp.dot(block, wout_v[h * value_size : (h + 1) * value_size, :], preferred_element_type=F32)
        attn = one if attn is None else attn + one
    abuf[tp] = attn.astype(BF16)
    attn_mix, gone = tp_total(abuf, asend, arecv)
    middle = (tok_v[...].astype(F32) + attn_mix).astype(BF16)
    mid_v[...] = middle
    mid = middle.astype(F32)
    squares = jnp.sum(mid * mid, axis=1, keepdims=True)
    normed = (mid * gain2_ref[...]).astype(BF16)
    put_part(square_rs.part, jnp.broadcast_to(squares, (batch, LANES)), 0, LANES)
    square_rs.first()
    late[1].wait()
    late[2].wait()
    for k, (at, wide) in enumerate(spans):
        half = padded(wide)
        for j, weight in enumerate([wgf_v, wuf_v]):
            out = lax.dot_general(
                normed, weight[at : at + wide, :], (((1,), (1,)), ((), ())), preferred_element_type=F32
            )
            put_part(ffn_rs[k].part, out, j * half, wide)
            if half > wide:
                fill = jnp.zeros((batch, half - wide), F32)
                put_part(ffn_rs[k].part, fill, j * half + wide, half - wide)
        ffn_rs[k].first()
    square_rs.second()
    late[3].wait()
    scale2 = None
    for kind, k in ffn_order(len(spans)):
        at, wide = spans[k]
        half = padded(wide)
        if kind == 0:
            ffn_rs[k].second()
        elif kind == 1:
            if scale2 is None:
                total = square_rs.total()
                scale2 = lax.rsqrt(total[:, :1] / (width * count) + norm_floor)
            both = ffn_rs[k].total() * scale2
            gate = both[:, :wide]
            up = both[:, half : half + wide]
            hid = gate / (1.0 + jnp.exp(-gate)) * up
            ffn_ag[k].buf[outer_at, inner_at] = hid.astype(BF16)
            ffn_ag[k].send()
        elif kind == 2:
            ffn_ag[k].relay()
        else:
            ffn_ag[k].wait()
            hid = ffn_ag[k].buf[...].astype(F32).reshape(batch, wide).astype(BF16)
            one = jnp.dot(hid, wdf_v[at : at + wide, :], preferred_element_type=F32)
            if k == 0:
                acc_v[...] = one
            else:
                acc_v[...] += one
    dbuf[tp] = acc_v[...].astype(BF16)
    down, copies = tp_total(dbuf, dsend, drecv)
    mixed_ref[...] = (mid_v[...].astype(F32) + down).astype(BF16)
    gone += copies
    for group in [gates_rs, *proj_rs, *head_ag, square_rs, *ffn_rs, *ffn_ag]:
        gone += group.gone
    for copy in gone:
        copy.wait_send()


def store_kernel(mixed_in, c_in, n_in, m_in, mixed_out, c_out, n_out, m_out, sems):
    rows = c_in.shape[0]
    copies = [pltpu.make_async_copy(c_in.at[b], c_out.at[b], sems.at[b]) for b in range(rows)]
    copies += [
        pltpu.make_async_copy(src, dst, sems.at[rows + i])
        for i, (src, dst) in enumerate([(mixed_in, mixed_out), (n_in, n_out), (m_in, m_out)])
    ]
    for copy in copies:
        copy.start()
    for copy in copies:
        copy.wait()


def per_device(
    tokens,
    attn_gain,
    w_query,
    w_key,
    w_value,
    w_outgate,
    w_gates,
    forget_bias,
    state_c,
    state_n,
    state_m,
    w_output,
    mlp_gain,
    w_gateff,
    w_upff,
    w_downff,
):
    count = lax.axis_size("kv")
    tps = lax.axis_size("tp")
    batch, width = tokens.shape
    rows, heads, value_size, query_size = state_c.shape
    hidden = w_gateff.shape[1]
    inner = inner_size(count)
    outer = count // inner
    spans = hidden_spans(hidden)
    sem = pltpu.SemaphoreType.DMA
    struct = jax.ShapeDtypeStruct
    args = (
        tokens, attn_gain[None], w_query, w_key, w_value, w_outgate, w_gates.T,
        forget_bias[None], state_m.T, state_n, state_c, w_output, mlp_gain[None],
        w_gateff.T, w_upff.T, w_downff,
    )
    chunks = [heads * query_size] * 2 + [value_size] * (2 * heads)
    scratch = [
        pltpu.VMEM(tokens.shape, BF16),
        pltpu.VMEM((1, width), F32),
        *[pltpu.VMEM(w.shape, BF16) for w in (w_query, w_key, w_value, w_outgate)],
        pltpu.VMEM((w_gates.shape[1], width), BF16),
        *[pltpu.VMEM(w.shape, BF16) for w in (w_output, w_gateff.T, w_upff.T, w_downff)],
        *[pltpu.VMEM(args[i].shape, F32) for i in (7, 8, 9, 12)],
        sem((7 + len(chunks),)),
        sem((rows, heads)),
        sem((4,)),
    ]
    scratch += scatter_scratch(inner, outer, rows, LANES, F32)
    for wide in chunks:
        scratch += scatter_scratch(inner, outer, rows, wide, BF16)
    for _ in range(heads):
        scratch += gather_scratch(inner, outer, rows, value_size)
    for _, wide in spans:
        scratch += scatter_scratch(inner, outer, rows, 2 * padded(wide), BF16)
    scratch += scatter_scratch(inner, outer, rows, LANES, F32)
    for _, wide in spans:
        scratch += gather_scratch(inner, outer, rows, wide)
    scratch += [
        pltpu.VMEM((tps, batch, width), BF16),
        pltpu.VMEM((tps, batch, width), BF16),
        pltpu.VMEM((batch, width), BF16),
        pltpu.VMEM((batch, width), F32),
        pltpu.VMEM((heads, value_size, rows), F32),
        *[sem((tps,))] * 4,
    ]

    def kernel(*refs):
        layer_kernel(heads, spans, *refs)

    kernel_outs = (
        struct((batch, width), BF16),
        struct(state_c.shape, F32),
        struct(state_n.shape, F32),
        struct(state_m.T.shape, F32),
    )
    state_bytes = state_c.size * 4
    outs = pl.pallas_call(
        kernel,
        out_shape=kernel_outs,
        in_specs=[HBM_SPEC] * len(args),
        out_specs=(VMEM_SPEC,) * 4,
        scratch_shapes=scratch,
        compiler_params=pltpu.CompilerParams(
            collective_id=0, has_side_effects=True,
            vmem_limit_bytes=VMEM_ALL - state_bytes - ROOM,
        ),
        name="layer",
    )(*[pltpu.with_memory_space_constraint(arg, pltpu.HBM) for arg in args])
    mixed, new_c, new_n, new_m = pl.pallas_call(
        store_kernel,
        out_shape=kernel_outs,
        in_specs=[VMEM_SPEC] * 4,
        out_specs=(HBM_SPEC,) * 4,
        scratch_shapes=[sem((rows + 3,))],
        compiler_params=pltpu.CompilerParams(vmem_limit_bytes=ROOM),
        name="store",
    )(*outs)
    return (mixed, new_c, new_n, new_m.T)


def solution(mesh):
    placed = (
        P(None, "kv"),
        P("kv"),
        P("kv", "tp"),
        P("kv", "tp"),
        P("kv", "tp"),
        P("kv", "tp"),
        P(),
        P(),
        P("kv", "tp", None, None),
        P("kv", "tp", None),
        P("kv", "tp"),
        P("tp", "kv"),
        P("kv"),
        P("kv", "tp"),
        P("kv", "tp"),
        P("tp", "kv"),
    )
    return jax.shard_map(
        per_device,
        mesh=mesh,
        in_specs=placed,
        out_specs=(P(None, "kv"), P("kv", "tp", None, None), P("kv", "tp", None), P("kv", "tp")),
        check_vma=False,
    )
```

```python
import jax
import jax.numpy as jnp
from jax import lax
from jax.experimental import pallas as pl
from jax.experimental.pallas import tpu as pltpu
from jax.sharding import PartitionSpec as P

norm_floor = 1e-05
MESH = pl.DeviceIdType.MESH
LANES = 128
SPAN = 512
EDGE = 256
WINDOW = 3
VMEM_ALL = 67043328
ROOM = 4 * 1024 * 1024
VMEM_SPEC = pl.BlockSpec(memory_space=pltpu.VMEM)
HBM_SPEC = pl.BlockSpec(memory_space=pltpu.HBM)
F32, BF16 = jnp.float32, jnp.bfloat16


def peer_of(axis, step):
    count = lax.axis_size(axis)
    return lax.rem(lax.axis_index(axis) + step, count)


def signal_peers(barrier, axis):
    for step in range(1, lax.axis_size(axis)):
        pl.semaphore_signal(
            barrier, inc=1, device_id={axis: peer_of(axis, step)}, device_id_type=MESH
        )


def inner_size(count):
    size = 1 << ((count.bit_length() - 1) // 2)
    return size if count % size == 0 else 1


def place():
    count = lax.axis_size("kv")
    inner = inner_size(count)
    kv = lax.axis_index("kv")
    return kv // inner, kv % inner, count // inner, inner


def inner_peer(step):
    outer_at, inner_at, _, inner = place()
    return (inner_at + step) % inner, outer_at * inner + (inner_at + step) % inner


def outer_peer(step):
    outer_at, inner_at, outer, inner = place()
    return (outer_at + step) % outer, ((outer_at + step) % outer) * inner + inner_at


def remote_copy(axis, device, src, dst, send_sem, recv_sem):
    return pltpu.make_async_remote_copy(
        src_ref=src,
        dst_ref=dst,
        send_sem=send_sem,
        recv_sem=recv_sem,
        device_id={axis: device},
        device_id_type=MESH,
    )


def send_to(axis, device, src, dst, send_sem, recv_sem):
    copy = remote_copy(axis, device, src, dst, send_sem, recv_sem)
    copy.start()
    return copy


def put_part(part, out, at, size):
    inner, outer, rows, _ = part.shape
    split = out.reshape(outer, inner, rows, size).astype(part.dtype)
    for i in range(inner):
        part[i, :, :, at : at + size] = split[:, i]


class Scatter:
    def __init__(self, part, land, both, last, esend, erecv, fsend, frecv):
        self.part, self.land, self.both, self.last = part, land, both, last
        self.esend, self.erecv, self.fsend, self.frecv = esend, erecv, fsend, frecv
        self.gone = []

    def one(self):
        copies = []
        for step in range(1, self.part.shape[0]):
            at, device = inner_peer(step)
            copies.append(
                remote_copy(
                    "kv", device, self.part.at[at], self.land.at[step],
                    self.esend.at[step], self.erecv.at[step],
                )
            )
        return copies

    def second(self):
        _, inner_at, outer, inner = place()
        for copy in self.one():
            copy.wait_recv()
        acc = self.part[inner_at].astype(F32)
        for step in range(1, inner):
            acc += self.land[step].astype(F32)
        self.both[...] = acc.astype(self.both.dtype)
        self.two = []
        for step in range(1, outer):
            to, device = outer_peer(step)
            self.two.append(
                send_to(
                    "kv", device, self.both.at[to], self.last.at[step],
                    self.fsend.at[step], self.frecv.at[step],
                )
            )
        self.gone += self.two

    def total(self):
        outer_at, _, outer, _ = place()
        for copy in self.two:
            copy.wait_recv()
        acc = self.both[outer_at].astype(F32)
        for step in range(1, outer):
            acc += self.last[step].astype(F32)
        return acc


def scatter_scratch(inner, outer, rows, wide, dtype):
    sem = pltpu.SemaphoreType.DMA
    return [
        pltpu.VMEM((inner, outer, rows, wide), dtype),
        pltpu.VMEM((inner, outer, rows, wide), dtype),
        pltpu.VMEM((outer, rows, wide), dtype),
        pltpu.VMEM((outer, rows, wide), dtype),
        sem((inner,)),
        sem((inner,)),
        sem((outer,)),
        sem((outer,)),
    ]


class Gather:
    def __init__(self, buf, asend, arecv, bsend, brecv):
        self.buf = buf
        self.asend, self.arecv, self.bsend, self.brecv = asend, arecv, bsend, brecv
        self.gone = []

    def send(self):
        outer_at, inner_at, outer, inner = place()
        own = self.buf.at[outer_at, inner_at]
        self.along = []
        self.across = []
        for step in range(1, outer):
            self.along.append(
                send_to("kv", outer_peer(step)[1], own, own, self.asend.at[step], self.arecv.at[step])
            )
        self._across(0)
        self.gone += self.along

    def _across(self, far):
        outer_at, inner_at, outer, inner = place()
        block = self.buf.at[(outer_at + outer - far) % outer, inner_at]
        for step in range(1, inner):
            copy = send_to(
                "kv", inner_peer(step)[1], block, block, self.bsend.at[far, step], self.brecv.at[far, step]
            )
            self.across.append(copy)
            self.gone.append(copy)

    def relay(self):
        for far, copy in enumerate(self.along):
            copy.wait_recv()
            self._across(far + 1)

    def wait(self):
        for copy in self.across:
            copy.wait_recv()


def gather_scratch(inner, outer, rows, wide):
    sem = pltpu.SemaphoreType.DMA
    return [
        pltpu.VMEM((outer, inner, rows, wide), BF16),
        sem((outer,)),
        sem((outer,)),
        sem((outer, inner)),
        sem((outer, inner)),
    ]


def tp_total(buf, send_sem, recv_sem):
    tp = lax.axis_index("tp")
    count = lax.axis_size("tp")
    copies = [
        send_to("tp", peer_of("tp", step), buf.at[tp], buf.at[tp], send_sem.at[step], recv_sem.at[step])
        for step in range(1, count)
    ]
    for copy in copies:
        copy.wait_recv()
    total = buf[0].astype(F32)
    for i in range(1, count):
        total += buf[i].astype(F32)
    return total, copies


class Queue:
    def __init__(self, scatters, turn):
        self.scatters, self.turn = scatters, turn
        self.tp = lax.axis_index("tp")
        self.paired = lax.axis_size("tp") % 2 == 0

    def _issue(self, k):
        if k >= WINDOW:
            for copy in self.scatters[k - WINDOW].one():
                copy.wait_send()
        for copy in self.scatters[k].one():
            copy.start()

    def early(self, k):
        if not self.paired:
            self._issue(k)
            return

        @pl.when(self.tp % 2 == 0)
        def _():
            self._issue(k)
            if k == max(len(self.scatters) - 2, 0):
                pl.semaphore_signal(self.turn, inc=1, device_id={"tp": self.tp + 1}, device_id_type=MESH)

    def late(self):
        if not self.paired:
            return

        @pl.when(self.tp % 2 == 1)
        def _():
            pl.semaphore_wait(self.turn, 1)
            for k in range(len(self.scatters)):
                self._issue(k)

    def finish(self):
        for scatter in self.scatters[-WINDOW:]:
            for copy in scatter.one():
                copy.wait_send()


def padded(wide):
    return -(-wide // LANES) * LANES


def hidden_spans(hidden):
    sizes = [min(EDGE, hidden)]
    while hidden - sum(sizes) >= SPAN + EDGE:
        sizes.append(SPAN)
    while hidden > sum(sizes):
        sizes.append(min(EDGE, hidden - sum(sizes)))
    return [(sum(sizes[:k]), wide) for k, wide in enumerate(sizes)]


def ffn_order(spans):
    hidden = spans[-1][0] + spans[-1][1]
    events = []
    for k, (at, wide) in enumerate(spans):
        sent = 4.0 * (at + wide) / hidden
        own = 4.0 * wide / hidden
        second = sent + 2.6
        total = second + 4.0 + own
        relay = total + 4.0 + own / 2
        events += [(at / hidden, 0, k), (second, 1, k), (total, 2, k), (relay, 3, k), (relay + 2.6 + own / 2, 4, k)]
    return [(kind, k) for _, kind, k in sorted(events)]


def layer_kernel(heads, spans, *refs):
    (
        tok_hbm, gain1_hbm, wq, wk, wv, wo, wg, bias_hbm, m_hbm, n_hbm, c_hbm, wout, gain2_hbm, wgf, wuf, wdf,
        mixed_ref, newc_ref, newn_ref, newm_ref,
    ) = refs[:20]
    scratch = list(refs[20:])

    def take(n):
        got = scratch[:n]
        del scratch[:n]
        return got

    tok_v, gain1_v, wq_v, wk_v, wv_v, wo_v, wg_v, wout_v, wgf_v, wuf_v, wdf_v = take(11)
    bias_ref, m_ref, n_ref, gain2_ref, clow = take(5)
    wload, cload, sload = take(3)
    gates_rs = Scatter(*take(8))
    proj_rs = [Scatter(*take(8)) for _ in range(2 + 2 * heads)]
    head_ag = [Gather(*take(5)) for _ in range(heads)]
    ffn_rs = [Scatter(*take(8)) for _ in spans]
    square_rs = Scatter(*take(8))
    ffn_ag = [Gather(*take(5)) for _ in spans]
    abuf, dbuf, mid_v, acc_v, cols_v, asend, arecv, dsend, drecv, turn = take(10)

    kv = lax.axis_index("kv")
    tp = lax.axis_index("tp")
    count = lax.axis_size("kv")
    outer_at, inner_at, outer, inner = place()
    batch, width = tok_v.shape
    rows = batch // count
    _, _, value_size, query_size = newc_ref.shape
    heads_all = bias_ref.shape[1]
    gate_cols = wg_v.shape[0]

    barrier = pltpu.get_barrier_semaphore()
    signal_peers(barrier, "kv")
    signal_peers(barrier, "tp")
    chunks = [(wq, wq_v, 0, heads * query_size), (wk, wk_v, 0, heads * query_size)]
    for h in range(heads):
        chunks.append((wv, wv_v, h * value_size, value_size))
        chunks.append((wo, wo_v, h * value_size, value_size))
    early = [
        pltpu.make_async_copy(tok_hbm, tok_v, wload.at[0]),
        pltpu.make_async_copy(gain1_hbm, gain1_v, wload.at[1]),
        pltpu.make_async_copy(
            wg.at[:, pl.ds(pl.multiple_of(kv * width, LANES), width)], wg_v, wload.at[2]
        ),
    ]
    for load in early:
        load.start()
    small = [
        pltpu.make_async_copy(src, dst, sload.at[i])
        for i, (src, dst) in enumerate(
            [(bias_hbm, bias_ref), (m_hbm, m_ref), (n_hbm, n_ref), (gain2_hbm, gain2_ref)]
        )
    ]
    for load in small:
        load.start()
    loads = []
    for i, (src, dst, at, wide) in enumerate(chunks):
        load = pltpu.make_async_copy(
            src.at[:, pl.ds(at, wide)], dst.at[:, pl.ds(at, wide)], wload.at[7 + i]
        )
        load.start()
        loads.append(load)
    early[0].wait()
    early[1].wait()
    tok = tok_v[...].astype(F32)
    squares = jnp.sum(tok * tok, axis=1, keepdims=True)
    normed = (tok * gain1_v[...]).astype(BF16)
    proj_queue = Queue([proj_rs[0], gates_rs, *proj_rs[1:]], turn.at[0])
    for load in loads:
        load.wait()
    cloads = [
        [pltpu.make_async_copy(c_hbm.at[b, h], newc_ref.at[b, h], cload.at[b, h]) for b in range(rows)]
        for h in range(heads)
    ]
    for group in cloads:
        for load in group:
            load.start()
    late = [
        pltpu.make_async_copy(src, dst, wload.at[3 + i])
        for i, (src, dst) in enumerate([(wout, wout_v), (wgf, wgf_v), (wuf, wuf_v), (wdf, wdf_v)])
    ]
    for load in late:
        load.start()
    for i, (_, dst, at, wide) in enumerate(chunks):
        out = jnp.dot(normed, dst[:, at : at + wide], preferred_element_type=F32)
        put_part(proj_rs[i].part, out, 0, wide)
        if i == 1:
            early[2].wait()
            gates = lax.dot_general(
                normed, wg_v[...], (((1,), (1,)), ((), ())), preferred_element_type=F32
            )
            put_part(gates_rs.part, jnp.broadcast_to(squares, (batch, LANES)), 0, LANES)
            put_part(gates_rs.part, gates, 0, gate_cols)
            pl.semaphore_wait(barrier, count - 1 + lax.axis_size("tp") - 1)
            for j in range(3):
                proj_queue.early(j)
        elif i > 1:
            proj_queue.early(i + 1)
    proj_queue.late()
    for load in small:
        load.wait()
    proj_rs[0].second()
    gates_rs.second()
    for rs in proj_rs[1:]:
        rs.second()

    for h in range(heads):
        for b in range(rows):
            cloads[h][b].wait()
    for h in range(heads):
        for b in range(rows):
            clow[b, h] = newc_ref[b, h].astype(BF16)
    scale_query = proj_rs[0].total()
    gate_sum = gates_rs.total()
    scale = lax.rsqrt(gate_sum[:, gate_cols : gate_cols + 1] / (width * count) + norm_floor)
    gates = gate_sum * scale
    query_all = scale_query * (scale * query_size ** (-0.5))
    query_low = query_all.astype(BF16)
    lane = lax.broadcasted_iota(jnp.int32, gates.shape, 1)
    bias_lane = lax.broadcasted_iota(jnp.int32, bias_ref.shape, 1)
    sub = lax.broadcasted_iota(jnp.int32, (rows, value_size), 0)
    eye = lax.broadcasted_iota(jnp.int32, (rows, rows), 0) == lax.broadcasted_iota(
        jnp.int32, (rows, rows), 1
    )
    keeps, admits, new_ms = [], [], []
    for h in range(heads):
        column = tp * heads + h
        log_input = jnp.sum(jnp.where(lane == column, gates, 0.0), axis=1, keepdims=True)
        forget = jnp.sum(jnp.where(lane == heads_all + column, gates, 0.0), axis=1, keepdims=True)
        bias = jnp.sum(jnp.where(bias_lane == column, bias_ref[...], 0.0), axis=1, keepdims=True)
        pre = forget + bias
        log_forget = jnp.minimum(pre, 0.0) - jnp.log(1.0 + jnp.exp(-jnp.abs(pre)))
        old_m = jnp.sum(jnp.where(eye, m_ref[h : h + 1, :], 0.0), axis=1, keepdims=True)
        carried = log_forget + old_m
        new_m = jnp.maximum(carried, log_input)
        keeps.append(jnp.exp(carried - new_m))
        admits.append(jnp.exp(log_input - new_m))
        new_ms.append(new_m)
        newm_ref[h : h + 1, :] = jnp.sum(jnp.where(eye, new_m, 0.0), axis=0, keepdims=True)
    reads = []
    for h in range(heads):
        read = jnp.zeros((rows, value_size), F32)
        low = query_low[:, h * query_size : (h + 1) * query_size]
        for b in range(rows):
            one = lax.dot_general(
                low, clow[b, h], (((1,), (1,)), ((), ())), preferred_element_type=F32
            )
            read = jnp.where(sub == b, one, read)
        reads.append(read)
    key_all = proj_rs[1].total() * scale
    keys = []
    for h in range(heads):
        query = query_all[:, h * query_size : (h + 1) * query_size]
        key = admits[h] * key_all[:, h * query_size : (h + 1) * query_size]
        keys.append(key)
        new_n = keeps[h] * n_ref[:, h, :] + key
        newn_ref[:, h, :] = new_n
        denom = jnp.maximum(
            jnp.abs(jnp.sum(new_n * query, axis=1, keepdims=True)), jnp.exp(-new_ms[h])
        )
        value = proj_rs[2 + 2 * h].total() * scale
        numer = keeps[h] * reads[h] + value * jnp.sum(key * query, axis=1, keepdims=True)
        cols_v[h] = value.T
        out_pre = proj_rs[3 + 2 * h].total() * scale
        gated = numer / ((1.0 + jnp.exp(-out_pre)) * denom)
        head_ag[h].buf[outer_at, inner_at] = gated.astype(BF16)
        head_ag[h].send()
    for h in range(heads):
        keep_wide = jnp.broadcast_to(keeps[h], (rows, query_size))
        for b in range(rows):
            newc_ref[b, h] = (
                keep_wide[b : b + 1, :] * newc_ref[b, h] + cols_v[h, :, b : b + 1] * keys[h][b : b + 1, :]
            )
        if h == 0:
            for ag in head_ag:
                ag.relay()

    late[0].wait()
    attn = None
    for h in range(heads):
        head_ag[h].wait()
        block = head_ag[h].buf[...].astype(F32).reshape(batch, value_size).astype(BF16)
        one = jnp.dot(block, wout_v[h * value_size : (h + 1) * value_size, :], preferred_element_type=F32)
        attn = one if attn is None else attn + one
    abuf[tp] = attn.astype(BF16)
    attn_mix, gone = tp_total(abuf, asend, arecv)
    middle = (tok_v[...].astype(F32) + attn_mix).astype(BF16)
    mid_v[...] = middle
    mid = middle.astype(F32)
    squares = jnp.sum(mid * mid, axis=1, keepdims=True)
    normed = (mid * gain2_ref[...]).astype(BF16)
    put_part(square_rs.part, jnp.broadcast_to(squares, (batch, LANES)), 0, LANES)
    late[1].wait()
    late[2].wait()
    ffn_queue = Queue([square_rs, *ffn_rs], turn.at[1])
    scale2 = None
    for kind, k in ffn_order(spans):
        at, wide = spans[k]
        half = padded(wide)
        if kind == 0:
            for j, weight in enumerate([wgf_v, wuf_v]):
                out = lax.dot_general(
                    normed, weight[at : at + wide, :], (((1,), (1,)), ((), ())), preferred_element_type=F32
                )
                put_part(ffn_rs[k].part, out, j * half, wide)
                if half > wide:
                    fill = jnp.zeros((batch, half - wide), F32)
                    put_part(ffn_rs[k].part, fill, j * half + wide, half - wide)
            if k == 0:
                ffn_queue.early(0)
            ffn_queue.early(k + 1)
            if k == len(spans) - 1:
                ffn_queue.late()
        elif kind == 1:
            ffn_rs[k].second()
            if k == 0:
                square_rs.second()
        elif kind == 2:
            if scale2 is None:
                total = square_rs.total()
                scale2 = lax.rsqrt(total[:, :1] / (width * count) + norm_floor)
            both = ffn_rs[k].total() * scale2
            gate = both[:, :wide]
            up = both[:, half : half + wide]
            hid = gate / (1.0 + jnp.exp(-gate)) * up
            ffn_ag[k].buf[outer_at, inner_at] = hid.astype(BF16)
            ffn_ag[k].send()
        elif kind == 3:
            ffn_ag[k].relay()
        else:
            ffn_ag[k].wait()
            if k == 0:
                late[3].wait()
            hid = ffn_ag[k].buf[...].astype(F32).reshape(batch, wide).astype(BF16)
            one = jnp.dot(hid, wdf_v[at : at + wide, :], preferred_element_type=F32)
            if k == 0:
                acc_v[...] = one
            else:
                acc_v[...] += one
    dbuf[tp] = acc_v[...].astype(BF16)
    down, copies = tp_total(dbuf, dsend, drecv)
    mixed_ref[...] = (mid_v[...].astype(F32) + down).astype(BF16)
    gone += copies
    for group in [gates_rs, *proj_rs, *head_ag, square_rs, *ffn_rs, *ffn_ag]:
        gone += group.gone
    proj_queue.finish()
    ffn_queue.finish()
    for copy in gone:
        copy.wait_send()


def store_kernel(mixed_in, c_in, n_in, m_in, mixed_out, c_out, n_out, m_out, sems):
    rows = c_in.shape[0]
    copies = [pltpu.make_async_copy(c_in.at[b], c_out.at[b], sems.at[b]) for b in range(rows)]
    copies += [
        pltpu.make_async_copy(src, dst, sems.at[rows + i])
        for i, (src, dst) in enumerate([(mixed_in, mixed_out), (n_in, n_out), (m_in, m_out)])
    ]
    for copy in copies:
        copy.start()
    for copy in copies:
        copy.wait()


def per_device(
    tokens,
    attn_gain,
    w_query,
    w_key,
    w_value,
    w_outgate,
    w_gates,
    forget_bias,
    state_c,
    state_n,
    state_m,
    w_output,
    mlp_gain,
    w_gateff,
    w_upff,
    w_downff,
):
    count = lax.axis_size("kv")
    tps = lax.axis_size("tp")
    batch, width = tokens.shape
    rows, heads, value_size, query_size = state_c.shape
    hidden = w_gateff.shape[1]
    inner = inner_size(count)
    outer = count // inner
    spans = hidden_spans(hidden)
    sem = pltpu.SemaphoreType.DMA
    struct = jax.ShapeDtypeStruct
    args = (
        tokens, attn_gain[None], w_query, w_key, w_value, w_outgate, w_gates.T,
        forget_bias[None], state_m.T, state_n, state_c, w_output, mlp_gain[None],
        w_gateff.T, w_upff.T, w_downff,
    )
    chunks = [heads * query_size] * 2 + [value_size] * (2 * heads)
    scratch = [
        pltpu.VMEM(tokens.shape, BF16),
        pltpu.VMEM((1, width), F32),
        *[pltpu.VMEM(w.shape, BF16) for w in (w_query, w_key, w_value, w_outgate)],
        pltpu.VMEM((w_gates.shape[1], width), BF16),
        *[pltpu.VMEM(w.shape, BF16) for w in (w_output, w_gateff.T, w_upff.T, w_downff)],
        *[pltpu.VMEM(args[i].shape, F32) for i in (7, 8, 9, 12)],
        pltpu.VMEM(state_c.shape, BF16),
        sem((7 + len(chunks),)),
        sem((rows, heads)),
        sem((4,)),
    ]
    scratch += scatter_scratch(inner, outer, rows, LANES, F32)
    for wide in chunks:
        scratch += scatter_scratch(inner, outer, rows, wide, BF16)
    for _ in range(heads):
        scratch += gather_scratch(inner, outer, rows, value_size)
    for _, wide in spans:
        scratch += scatter_scratch(inner, outer, rows, 2 * padded(wide), BF16)
    scratch += scatter_scratch(inner, outer, rows, LANES, F32)
    for _, wide in spans:
        scratch += gather_scratch(inner, outer, rows, wide)
    scratch += [
        pltpu.VMEM((tps, batch, width), BF16),
        pltpu.VMEM((tps, batch, width), BF16),
        pltpu.VMEM((batch, width), BF16),
        pltpu.VMEM((batch, width), F32),
        pltpu.VMEM((heads, value_size, rows), F32),
        *[sem((tps,))] * 4,
        pltpu.SemaphoreType.REGULAR((2,)),
    ]

    def kernel(*refs):
        layer_kernel(heads, spans, *refs)

    kernel_outs = (
        struct((batch, width), BF16),
        struct(state_c.shape, F32),
        struct(state_n.shape, F32),
        struct(state_m.T.shape, F32),
    )
    state_bytes = state_c.size * 4
    outs = pl.pallas_call(
        kernel,
        out_shape=kernel_outs,
        in_specs=[HBM_SPEC] * len(args),
        out_specs=(VMEM_SPEC,) * 4,
        scratch_shapes=scratch,
        compiler_params=pltpu.CompilerParams(
            collective_id=0, has_side_effects=True,
            vmem_limit_bytes=VMEM_ALL - 3 * state_bytes,
        ),
        name="layer",
    )(*[pltpu.with_memory_space_constraint(arg, pltpu.HBM) for arg in args])
    mixed, new_c, new_n, new_m = pl.pallas_call(
        store_kernel,
        out_shape=kernel_outs,
        in_specs=[VMEM_SPEC] * 4,
        out_specs=(HBM_SPEC,) * 4,
        scratch_shapes=[sem((rows + 3,))],
        compiler_params=pltpu.CompilerParams(vmem_limit_bytes=ROOM),
        name="store",
    )(*outs)
    return (mixed, new_c, new_n, new_m.T)


def solution(mesh):
    placed = (
        P(None, "kv"),
        P("kv"),
        P("kv", "tp"),
        P("kv", "tp"),
        P("kv", "tp"),
        P("kv", "tp"),
        P(),
        P(),
        P("kv", "tp", None, None),
        P("kv", "tp", None),
        P("kv", "tp"),
        P("tp", "kv"),
        P("kv"),
        P("kv", "tp"),
        P("kv", "tp"),
        P("tp", "kv"),
    )
    return jax.shard_map(
        per_device,
        mesh=mesh,
        in_specs=placed,
        out_specs=(P(None, "kv"), P("kv", "tp", None, None), P("kv", "tp", None), P("kv", "tp")),
        check_vma=False,
    )
```

```python
import jax
import jax.numpy as jnp
from jax import lax
from jax.experimental import pallas as pl
from jax.experimental.pallas import tpu as pltpu
from jax.sharding import PartitionSpec as P

norm_floor = 1e-05
MESH = pl.DeviceIdType.MESH
LANES = 128
SPAN = 512
EDGE = 256
PROJ_WINDOW, PROJ_HAND = 6, 2
FFN_WINDOW, FFN_HAND = 3, 3
VMEM_ALL = 67043328
ROOM = 4 * 1024 * 1024
VMEM_SPEC = pl.BlockSpec(memory_space=pltpu.VMEM)
HBM_SPEC = pl.BlockSpec(memory_space=pltpu.HBM)
F32, BF16 = jnp.float32, jnp.bfloat16


def peer_of(axis, step):
    count = lax.axis_size(axis)
    return lax.rem(lax.axis_index(axis) + step, count)


def signal_peers(barrier, axis):
    for step in range(1, lax.axis_size(axis)):
        pl.semaphore_signal(
            barrier, inc=1, device_id={axis: peer_of(axis, step)}, device_id_type=MESH
        )


def inner_size(count):
    size = 1 << ((count.bit_length() - 1) // 2)
    return size if count % size == 0 else 1


def place():
    count = lax.axis_size("kv")
    inner = inner_size(count)
    kv = lax.axis_index("kv")
    return kv // inner, kv % inner, count // inner, inner


def inner_peer(step):
    outer_at, inner_at, _, inner = place()
    return (inner_at + step) % inner, outer_at * inner + (inner_at + step) % inner


def outer_peer(step):
    outer_at, inner_at, outer, inner = place()
    return (outer_at + step) % outer, ((outer_at + step) % outer) * inner + inner_at


def remote_copy(axis, device, src, dst, send_sem, recv_sem):
    return pltpu.make_async_remote_copy(
        src_ref=src,
        dst_ref=dst,
        send_sem=send_sem,
        recv_sem=recv_sem,
        device_id={axis: device},
        device_id_type=MESH,
    )


def put_part(part, out, at, size):
    inner, outer, rows, _ = part.shape
    split = out.reshape(outer, inner, rows, size).astype(part.dtype)
    for i in range(inner):
        part[i, :, :, at : at + size] = split[:, i]


def wait_bytes(ref, sem):
    pltpu.make_async_copy(ref, ref, sem).wait()


class Scatter:
    def __init__(self, part, land, both, last, sems):
        self.part, self.land, self.both, self.last = part, land, both, last
        self.sems = sems

    def start(self):
        for step in range(1, self.part.shape[0]):
            at, device = inner_peer(step)
            remote_copy(
                "kv", device, self.part.at[at], self.land.at[step], self.sems.at[0], self.sems.at[1]
            ).start()

    def drain(self):
        if self.part.shape[0] > 1:
            wait_bytes(self.land.at[pl.ds(1, self.part.shape[0] - 1)], self.sems.at[0])

    def second(self):
        _, inner_at, outer, inner = place()
        if inner > 1:
            wait_bytes(self.land.at[pl.ds(1, inner - 1)], self.sems.at[1])
        acc = self.part[inner_at].astype(F32)
        for step in range(1, inner):
            acc += self.land[step].astype(F32)
        self.both[...] = acc.astype(self.both.dtype)
        for step in range(1, outer):
            to, device = outer_peer(step)
            remote_copy(
                "kv", device, self.both.at[to], self.last.at[step], self.sems.at[2], self.sems.at[3]
            ).start()

    def total(self):
        outer_at, _, outer, _ = place()
        wait_bytes(self.last.at[pl.ds(1, outer - 1)], self.sems.at[3])
        acc = self.both[outer_at].astype(F32)
        for step in range(1, outer):
            acc += self.last[step].astype(F32)
        return acc

    def settle(self):
        wait_bytes(self.last.at[pl.ds(1, self.last.shape[0] - 1)], self.sems.at[2])


def scatter_scratch(inner, outer, rows, wide, dtype):
    return [
        pltpu.VMEM((inner, outer, rows, wide), dtype),
        pltpu.VMEM((inner, outer, rows, wide), dtype),
        pltpu.VMEM((outer, rows, wide), dtype),
        pltpu.VMEM((outer, rows, wide), dtype),
        pltpu.SemaphoreType.DMA((4,)),
    ]


class Gather:
    def __init__(self, buf, sems):
        self.buf, self.sems = buf, sems

    def _across(self, far):
        outer_at, inner_at, outer, inner = place()
        block = self.buf.at[(outer_at + outer - far) % outer * inner + inner_at]
        for step in range(1, inner):
            remote_copy("kv", inner_peer(step)[1], block, block, self.sems.at[0], self.sems.at[2]).start()

    def send(self):
        outer = place()[2]
        own = self.buf.at[lax.axis_index("kv")]
        for step in range(outer - 1, 0, -1):
            remote_copy("kv", outer_peer(step)[1], own, own, self.sems.at[0], self.sems.at[1]).start()
        self._across(0)

    def relay(self):
        outer = place()[2]
        wait_bytes(self.buf.at[pl.ds(1, outer - 1)], self.sems.at[1])
        for far in range(1, outer):
            self._across(far)

    def wait(self):
        _, _, outer, inner = place()
        if inner > 1:
            wait_bytes(self.buf.at[pl.ds(0, outer * (inner - 1))], self.sems.at[2])

    def settle(self):
        wait_bytes(self.buf.at[pl.ds(1, self.buf.shape[0] - 1)], self.sems.at[0])


def gather_scratch(count, rows, wide):
    return [pltpu.VMEM((count, rows, wide), BF16), pltpu.SemaphoreType.DMA((3,))]


def tp_send(buf, sems):
    tp = lax.axis_index("tp")
    for step in range(1, buf.shape[0]):
        remote_copy("tp", peer_of("tp", step), buf.at[tp], buf.at[tp], sems.at[0], sems.at[1]).start()


def tp_total(buf, sems):
    wait_bytes(buf.at[pl.ds(1, buf.shape[0] - 1)], sems.at[1])
    total = buf[0].astype(F32)
    for i in range(1, buf.shape[0]):
        total += buf[i].astype(F32)
    return total


def tp_settle(buf, sems):
    wait_bytes(buf.at[pl.ds(1, buf.shape[0] - 1)], sems.at[0])


class Queue:
    def __init__(self, scatters, turn, window, hand):
        self.scatters, self.turn, self.window, self.hand = scatters, turn, window, max(len(scatters) - hand, 0)
        self.tp = lax.axis_index("tp")
        self.paired = lax.axis_size("tp") % 2 == 0

    def _issue(self, k):
        if k >= self.window:
            self.scatters[k - self.window].drain()
        self.scatters[k].start()

    def early(self, k):
        if not self.paired:
            self._issue(k)
            return

        @pl.when(self.tp % 2 == 0)
        def _():
            self._issue(k)
            if k == self.hand:
                pl.semaphore_signal(self.turn, inc=1, device_id={"tp": self.tp + 1}, device_id_type=MESH)

    def late(self):
        if not self.paired:
            return

        @pl.when(self.tp % 2 == 1)
        def _():
            pl.semaphore_wait(self.turn, 1)
            for k in range(len(self.scatters)):
                self._issue(k)

    def finish(self):
        for scatter in self.scatters[-self.window :]:
            scatter.drain()


def padded(wide):
    return -(-wide // LANES) * LANES


def hidden_spans(hidden):
    sizes = [min(EDGE, hidden)]
    while hidden - sum(sizes) >= SPAN + EDGE:
        sizes.append(SPAN)
    while hidden > sum(sizes):
        sizes.append(min(EDGE, hidden - sum(sizes)))
    return [(sum(sizes[:k]), wide) for k, wide in enumerate(sizes)]


def ffn_order(spans):
    hidden = spans[-1][0] + spans[-1][1]
    events = []
    for k, (at, wide) in enumerate(spans):
        sent = 4.0 * (at + wide) / hidden
        own = 4.0 * wide / hidden
        second = sent + 2.6
        total = second + 4.0 + own
        relay = total + 4.0 + own / 2
        events += [(at / hidden, 0, k), (second, 1, k), (total, 2, k), (relay, 3, k), (relay + 2.6 + own / 2, 4, k)]
    return [(kind, k) for _, kind, k in sorted(events)]


def layer_kernel(heads, spans, *refs):
    (
        tok_hbm, gain1_hbm, wq, wk, wv, wo, wg, bias_hbm, m_hbm, n_hbm, c_hbm, wout, gain2_hbm, wgf, wuf, wdf,
        mixed_ref, newc_ref, newn_ref, newm_ref,
    ) = refs[:20]
    scratch = list(refs[20:])

    def take(n):
        got = scratch[:n]
        del scratch[:n]
        return got

    tok_v, gain1_v, wq_v, wk_v, wv_v, wo_v, wg_v, wout_v, wgf_v, wuf_v, wdf_v = take(11)
    bias_ref, m_ref, n_ref, gain2_ref, clow = take(5)
    wload, cload, sload = take(3)
    gates_rs = Scatter(*take(5))
    proj_rs = [Scatter(*take(5)) for _ in range(2 + 2 * heads)]
    head_ag = [Gather(*take(2)) for _ in range(heads)]
    ffn_rs = [Scatter(*take(5)) for _ in spans]
    square_rs = Scatter(*take(5))
    ffn_ag = [Gather(*take(2)) for _ in spans]
    abuf, dbuf, mid_v, acc_v, cols_v, asem, dsem, turn = take(8)

    kv = lax.axis_index("kv")
    tp = lax.axis_index("tp")
    count = lax.axis_size("kv")
    outer_at, inner_at, outer, inner = place()
    batch, width = tok_v.shape
    rows = batch // count
    _, _, value_size, query_size = newc_ref.shape
    heads_all = bias_ref.shape[1]
    gate_cols = wg_v.shape[0]

    barrier = pltpu.get_barrier_semaphore()
    signal_peers(barrier, "kv")
    signal_peers(barrier, "tp")
    chunks = [(wq, wq_v, 0, heads * query_size), (wk, wk_v, 0, heads * query_size)]
    for h in range(heads):
        chunks.append((wv, wv_v, h * value_size, value_size))
        chunks.append((wo, wo_v, h * value_size, value_size))
    early = [
        pltpu.make_async_copy(tok_hbm, tok_v, wload.at[0]),
        pltpu.make_async_copy(gain1_hbm, gain1_v, wload.at[1]),
        pltpu.make_async_copy(
            wg.at[:, pl.ds(pl.multiple_of(kv * width, LANES), width)], wg_v, wload.at[2]
        ),
    ]
    for load in early:
        load.start()
    small = [
        pltpu.make_async_copy(src, dst, sload.at[i])
        for i, (src, dst) in enumerate(
            [(bias_hbm, bias_ref), (m_hbm, m_ref), (n_hbm, n_ref), (gain2_hbm, gain2_ref)]
        )
    ]
    for load in small:
        load.start()
    loads = []
    for i, (src, dst, at, wide) in enumerate(chunks):
        load = pltpu.make_async_copy(
            src.at[:, pl.ds(at, wide)], dst.at[:, pl.ds(at, wide)], wload.at[7 + i]
        )
        load.start()
        loads.append(load)
    early[0].wait()
    early[1].wait()
    tok = tok_v[...].astype(F32)
    normed = (tok * gain1_v[...]).astype(BF16)
    proj_queue = Queue([proj_rs[0], gates_rs, *proj_rs[1:]], turn.at[0], PROJ_WINDOW, PROJ_HAND)
    for i, (_, dst, at, wide) in enumerate(chunks):
        loads[i].wait()
        if i == len(chunks) - 1:
            for h in range(heads):
                for b in range(rows):
                    pltpu.make_async_copy(c_hbm.at[b, h], newc_ref.at[b, h], cload).start()
            late = [
                pltpu.make_async_copy(src, dst, wload.at[3 + i])
                for i, (src, dst) in enumerate([(wout, wout_v), (wgf, wgf_v), (wuf, wuf_v), (wdf, wdf_v)])
            ]
            for load in late:
                load.start()
        out = jnp.dot(normed, dst[:, at : at + wide], preferred_element_type=F32)
        put_part(proj_rs[i].part, out, 0, wide)
        if i == 0:
            pl.semaphore_wait(barrier, count - 1 + lax.axis_size("tp") - 1)
            proj_queue.early(0)
            early[2].wait()
            gates = lax.dot_general(
                normed, wg_v[...], (((1,), (1,)), ((), ())), preferred_element_type=F32
            )
            squares = jnp.sum(tok * tok, axis=1, keepdims=True)
            put_part(gates_rs.part, jnp.broadcast_to(squares, (batch, LANES)), 0, LANES)
            put_part(gates_rs.part, gates, 0, gate_cols)
            proj_queue.early(1)
        else:
            proj_queue.early(i + 1)
    proj_queue.late()
    for load in small:
        load.wait()
    proj_rs[0].second()
    gates_rs.second()
    for rs in proj_rs[1:]:
        rs.second()

    wait_bytes(newc_ref, cload)
    for h in range(heads):
        for b in range(rows):
            clow[b, h] = newc_ref[b, h].astype(BF16)
    scale_query = proj_rs[0].total()
    gate_sum = gates_rs.total()
    scale = lax.rsqrt(gate_sum[:, gate_cols : gate_cols + 1] / (width * count) + norm_floor)
    gates = gate_sum * scale
    query_all = scale_query * (scale * query_size ** (-0.5))
    query_low = query_all.astype(BF16)
    lane = lax.broadcasted_iota(jnp.int32, gates.shape, 1)
    bias_lane = lax.broadcasted_iota(jnp.int32, bias_ref.shape, 1)
    sub = lax.broadcasted_iota(jnp.int32, (rows, value_size), 0)
    eye = lax.broadcasted_iota(jnp.int32, (rows, rows), 0) == lax.broadcasted_iota(
        jnp.int32, (rows, rows), 1
    )
    keeps, admits, new_ms = [], [], []
    for h in range(heads):
        column = tp * heads + h
        log_input = jnp.sum(jnp.where(lane == column, gates, 0.0), axis=1, keepdims=True)
        forget = jnp.sum(jnp.where(lane == heads_all + column, gates, 0.0), axis=1, keepdims=True)
        bias = jnp.sum(jnp.where(bias_lane == column, bias_ref[...], 0.0), axis=1, keepdims=True)
        pre = forget + bias
        log_forget = jnp.minimum(pre, 0.0) - jnp.log(1.0 + jnp.exp(-jnp.abs(pre)))
        old_m = jnp.sum(jnp.where(eye, m_ref[h : h + 1, :], 0.0), axis=1, keepdims=True)
        carried = log_forget + old_m
        new_m = jnp.maximum(carried, log_input)
        keeps.append(jnp.exp(carried - new_m))
        admits.append(jnp.exp(log_input - new_m))
        new_ms.append(new_m)
        newm_ref[h : h + 1, :] = jnp.sum(jnp.where(eye, new_m, 0.0), axis=0, keepdims=True)
    reads = []
    for h in range(heads):
        read = jnp.zeros((rows, value_size), F32)
        low = query_low[:, h * query_size : (h + 1) * query_size]
        for b in range(rows):
            one = lax.dot_general(
                low, clow[b, h], (((1,), (1,)), ((), ())), preferred_element_type=F32
            )
            read = jnp.where(sub == b, one, read)
        reads.append(read)
    key_all = proj_rs[1].total() * scale
    keys = []
    for h in range(heads):
        query = query_all[:, h * query_size : (h + 1) * query_size]
        key = admits[h] * key_all[:, h * query_size : (h + 1) * query_size]
        keys.append(key)
        new_n = keeps[h] * n_ref[:, h, :] + key
        newn_ref[:, h, :] = new_n
        denom = jnp.maximum(
            jnp.abs(jnp.sum(new_n * query, axis=1, keepdims=True)), jnp.exp(-new_ms[h])
        )
        value = proj_rs[2 + 2 * h].total() * scale
        numer = keeps[h] * reads[h] + value * jnp.sum(key * query, axis=1, keepdims=True)
        cols_v[h] = value.T
        out_pre = proj_rs[3 + 2 * h].total() * scale
        gated = numer / ((1.0 + jnp.exp(-out_pre)) * denom)
        head_ag[h].buf[kv] = gated.astype(BF16)
        head_ag[h].send()
    for h in range(heads):
        keep_wide = jnp.broadcast_to(keeps[h], (rows, query_size))
        for b in range(rows):
            newc_ref[b, h] = (
                keep_wide[b : b + 1, :] * newc_ref[b, h] + cols_v[h, :, b : b + 1] * keys[h][b : b + 1, :]
            )
        if h == 0:
            for ag in head_ag:
                ag.relay()

    late[0].wait()
    attn = None
    for h in range(heads):
        head_ag[h].wait()
        block = head_ag[h].buf[...].astype(F32).reshape(batch, value_size).astype(BF16)
        one = jnp.dot(block, wout_v[h * value_size : (h + 1) * value_size, :], preferred_element_type=F32)
        attn = one if attn is None else attn + one
    abuf[tp] = attn.astype(BF16)
    tp_send(abuf, asem)
    for group in [gates_rs, *proj_rs, *head_ag]:
        group.settle()
    proj_queue.finish()
    attn_mix = tp_total(abuf, asem)
    middle = (tok_v[...].astype(F32) + attn_mix).astype(BF16)
    mid_v[...] = middle
    mid = middle.astype(F32)
    squares = jnp.sum(mid * mid, axis=1, keepdims=True)
    normed = (mid * gain2_ref[...]).astype(BF16)
    put_part(square_rs.part, jnp.broadcast_to(squares, (batch, LANES)), 0, LANES)
    late[1].wait()
    late[2].wait()
    ffn_queue = Queue([square_rs, *ffn_rs], turn.at[1], FFN_WINDOW, FFN_HAND)
    scale2 = None
    for kind, k in ffn_order(spans):
        at, wide = spans[k]
        half = padded(wide)
        if kind == 0:
            for j, weight in enumerate([wgf_v, wuf_v]):
                out = lax.dot_general(
                    normed, weight[at : at + wide, :], (((1,), (1,)), ((), ())), preferred_element_type=F32
                )
                put_part(ffn_rs[k].part, out, j * half, wide)
                if half > wide:
                    fill = jnp.zeros((batch, half - wide), F32)
                    put_part(ffn_rs[k].part, fill, j * half + wide, half - wide)
            if k == 0:
                ffn_queue.early(0)
            ffn_queue.early(k + 1)
            if k == len(spans) - 1:
                ffn_queue.late()
        elif kind == 1:
            ffn_rs[k].second()
            if k == 0:
                square_rs.second()
        elif kind == 2:
            if scale2 is None:
                total = square_rs.total()
                scale2 = lax.rsqrt(total[:, :1] / (width * count) + norm_floor)
            both = ffn_rs[k].total() * scale2
            gate = both[:, :wide]
            up = both[:, half : half + wide]
            hid = gate / (1.0 + jnp.exp(-gate)) * up
            ffn_ag[k].buf[kv] = hid.astype(BF16)
            ffn_ag[k].send()
        elif kind == 3:
            ffn_ag[k].relay()
        else:
            ffn_ag[k].wait()
            if k == 0:
                late[3].wait()
            hid = ffn_ag[k].buf[...].astype(F32).reshape(batch, wide).astype(BF16)
            one = jnp.dot(hid, wdf_v[at : at + wide, :], preferred_element_type=F32)
            if k == 0:
                acc_v[...] = one
            else:
                acc_v[...] += one
    dbuf[tp] = acc_v[...].astype(BF16)
    tp_send(dbuf, dsem)
    for group in [square_rs, *ffn_rs, *ffn_ag]:
        group.settle()
    ffn_queue.finish()
    tp_settle(abuf, asem)
    down = tp_total(dbuf, dsem)
    mixed_ref[...] = (mid_v[...].astype(F32) + down).astype(BF16)
    tp_settle(dbuf, dsem)


def store_kernel(mixed_in, c_in, n_in, m_in, mixed_out, c_out, n_out, m_out, sems):
    rows = c_in.shape[0]
    copies = [pltpu.make_async_copy(c_in.at[b], c_out.at[b], sems.at[b]) for b in range(rows)]
    copies += [
        pltpu.make_async_copy(src, dst, sems.at[rows + i])
        for i, (src, dst) in enumerate([(mixed_in, mixed_out), (n_in, n_out), (m_in, m_out)])
    ]
    for copy in copies:
        copy.start()
    for copy in copies:
        copy.wait()


def per_device(
    tokens,
    attn_gain,
    w_query,
    w_key,
    w_value,
    w_outgate,
    w_gates,
    forget_bias,
    state_c,
    state_n,
    state_m,
    w_output,
    mlp_gain,
    w_gateff,
    w_upff,
    w_downff,
):
    count = lax.axis_size("kv")
    tps = lax.axis_size("tp")
    batch, width = tokens.shape
    rows, heads, value_size, query_size = state_c.shape
    hidden = w_gateff.shape[1]
    inner = inner_size(count)
    outer = count // inner
    spans = hidden_spans(hidden)
    sem = pltpu.SemaphoreType.DMA
    struct = jax.ShapeDtypeStruct
    args = (
        tokens, attn_gain[None], w_query, w_key, w_value, w_outgate, w_gates.T,
        forget_bias[None], state_m.T, state_n, state_c, w_output, mlp_gain[None],
        w_gateff.T, w_upff.T, w_downff,
    )
    chunks = [heads * query_size] * 2 + [value_size] * (2 * heads)
    scratch = [
        pltpu.VMEM(tokens.shape, BF16),
        pltpu.VMEM((1, width), F32),
        *[pltpu.VMEM(w.shape, BF16) for w in (w_query, w_key, w_value, w_outgate)],
        pltpu.VMEM((w_gates.shape[1], width), BF16),
        *[pltpu.VMEM(w.shape, BF16) for w in (w_output, w_gateff.T, w_upff.T, w_downff)],
        *[pltpu.VMEM(args[i].shape, F32) for i in (7, 8, 9, 12)],
        pltpu.VMEM(state_c.shape, BF16),
        sem((7 + len(chunks),)),
        sem,
        sem((4,)),
    ]
    scratch += scatter_scratch(inner, outer, rows, LANES, F32)
    for wide in chunks:
        scratch += scatter_scratch(inner, outer, rows, wide, BF16)
    for _ in range(heads):
        scratch += gather_scratch(count, rows, value_size)
    for _, wide in spans:
        scratch += scatter_scratch(inner, outer, rows, 2 * padded(wide), BF16)
    scratch += scatter_scratch(inner, outer, rows, LANES, F32)
    for _, wide in spans:
        scratch += gather_scratch(count, rows, wide)
    scratch += [
        pltpu.VMEM((tps, batch, width), BF16),
        pltpu.VMEM((tps, batch, width), BF16),
        pltpu.VMEM((batch, width), BF16),
        pltpu.VMEM((batch, width), F32),
        pltpu.VMEM((heads, value_size, rows), F32),
        *[sem((2,))] * 2,
        pltpu.SemaphoreType.REGULAR((2,)),
    ]

    def kernel(*refs):
        layer_kernel(heads, spans, *refs)

    kernel_outs = (
        struct((batch, width), BF16),
        struct(state_c.shape, F32),
        struct(state_n.shape, F32),
        struct(state_m.T.shape, F32),
    )
    state_bytes = state_c.size * 4
    outs = pl.pallas_call(
        kernel,
        out_shape=kernel_outs,
        in_specs=[HBM_SPEC] * len(args),
        out_specs=(VMEM_SPEC,) * 4,
        scratch_shapes=scratch,
        compiler_params=pltpu.CompilerParams(
            collective_id=0, has_side_effects=True,
            vmem_limit_bytes=VMEM_ALL - 3 * state_bytes,
        ),
        name="layer",
    )(*[pltpu.with_memory_space_constraint(arg, pltpu.HBM) for arg in args])
    mixed, new_c, new_n, new_m = pl.pallas_call(
        store_kernel,
        out_shape=kernel_outs,
        in_specs=[VMEM_SPEC] * 4,
        out_specs=(HBM_SPEC,) * 4,
        scratch_shapes=[sem((rows + 3,))],
        compiler_params=pltpu.CompilerParams(vmem_limit_bytes=ROOM),
        name="store",
    )(*outs)
    return (mixed, new_c, new_n, new_m.T)


def solution(mesh):
    placed = (
        P(None, "kv"),
        P("kv"),
        P("kv", "tp"),
        P("kv", "tp"),
        P("kv", "tp"),
        P("kv", "tp"),
        P(),
        P(),
        P("kv", "tp", None, None),
        P("kv", "tp", None),
        P("kv", "tp"),
        P("tp", "kv"),
        P("kv"),
        P("kv", "tp"),
        P("kv", "tp"),
        P("tp", "kv"),
    )
    return jax.shard_map(
        per_device,
        mesh=mesh,
        in_specs=placed,
        out_specs=(P(None, "kv"), P("kv", "tp", None, None), P("kv", "tp", None), P("kv", "tp")),
        check_vma=False,
    )
```

```python
import jax
import jax.numpy as jnp
from jax import lax
from jax.experimental import pallas as pl
from jax.experimental.pallas import tpu as pltpu
from jax.sharding import PartitionSpec as P

norm_floor = 1e-05
MESH = pl.DeviceIdType.MESH
LANES = 128
SPAN = 512
EDGE = 256
PROJ_WINDOW, PROJ_HAND = 6, 2
FFN_WINDOW, FFN_HAND = 3, 1
OUTER_SPAN, OUTER_AT = 640, (1,)

VMEM_ALL = 67043328
ROOM = 4 * 1024 * 1024
VMEM_SPEC = pl.BlockSpec(memory_space=pltpu.VMEM)
HBM_SPEC = pl.BlockSpec(memory_space=pltpu.HBM)
F32, BF16 = jnp.float32, jnp.bfloat16


def peer_of(axis, step):
    count = lax.axis_size(axis)
    return lax.rem(lax.axis_index(axis) + step, count)


def signal_peers(barrier, axis):
    for step in range(1, lax.axis_size(axis)):
        pl.semaphore_signal(
            barrier, inc=1, device_id={axis: peer_of(axis, step)}, device_id_type=MESH
        )


def inner_size(count):
    size = 1 << ((count.bit_length() - 1) // 2)
    return size if count % size == 0 else 1


def place():
    count = lax.axis_size("kv")
    inner = inner_size(count)
    kv = lax.axis_index("kv")
    return kv // inner, kv % inner, count // inner, inner


def inner_peer(step):
    outer_at, inner_at, _, inner = place()
    return (inner_at + step) % inner, outer_at * inner + (inner_at + step) % inner


def outer_peer(step):
    outer_at, inner_at, outer, inner = place()
    return (outer_at + step) % outer, ((outer_at + step) % outer) * inner + inner_at


def remote_copy(axis, device, src, dst, send_sem, recv_sem):
    return pltpu.make_async_remote_copy(
        src_ref=src,
        dst_ref=dst,
        send_sem=send_sem,
        recv_sem=recv_sem,
        device_id={axis: device},
        device_id_type=MESH,
    )


def wait_bytes(ref, sem):
    pltpu.make_async_copy(ref, ref, sem).wait()


class Scatter:
    def __init__(self, part, land, both, last, sems, inner_first=True):
        self.part, self.land, self.both, self.last = part, land, both, last
        self.sems, self.inner_first = sems, inner_first
        self.firsts, self.seconds = part.shape[0], part.shape[1]

    def _peers(self):
        return (inner_peer, outer_peer) if self.inner_first else (outer_peer, inner_peer)

    def _places(self):
        outer_at, inner_at, _, _ = place()
        return (inner_at, outer_at) if self.inner_first else (outer_at, inner_at)

    def put(self, out, at, size):
        inner, outer = (self.firsts, self.seconds) if self.inner_first else (self.seconds, self.firsts)
        split = out.reshape(outer, inner, self.part.shape[2], size).astype(self.part.dtype)
        for i in range(self.firsts):
            self.part[i, :, :, at : at + size] = split[:, i] if self.inner_first else split[i]

    def start(self):
        for step in range(self.firsts - 1, 0, -1):
            at, device = self._peers()[0](step)
            remote_copy(
                "kv", device, self.part.at[at], self.land.at[step], self.sems.at[0], self.sems.at[1]
            ).start()

    def drain(self):
        if self.firsts > 1:
            wait_bytes(self.land.at[pl.ds(1, self.firsts - 1)], self.sems.at[0])

    def second(self):
        if self.firsts > 1:
            wait_bytes(self.land.at[pl.ds(1, self.firsts - 1)], self.sems.at[1])
        acc = self.part[self._places()[0]].astype(F32)
        for step in range(1, self.firsts):
            acc += self.land[step].astype(F32)
        self.both[...] = acc.astype(self.both.dtype)
        for step in range(1, self.seconds):
            to, device = self._peers()[1](step)
            remote_copy(
                "kv", device, self.both.at[to], self.last.at[step], self.sems.at[2], self.sems.at[3]
            ).start()

    def total(self):
        if self.seconds > 1:
            wait_bytes(self.last.at[pl.ds(1, self.seconds - 1)], self.sems.at[3])
        acc = self.both[self._places()[1]].astype(F32)
        for step in range(1, self.seconds):
            acc += self.last[step].astype(F32)
        return acc

    def settle(self):
        if self.seconds > 1:
            wait_bytes(self.last.at[pl.ds(1, self.seconds - 1)], self.sems.at[2])


def scatter_scratch(firsts, seconds, rows, wide, dtype):
    return [
        pltpu.VMEM((firsts, seconds, rows, wide), dtype),
        pltpu.VMEM((firsts, seconds, rows, wide), dtype),
        pltpu.VMEM((seconds, rows, wide), dtype),
        pltpu.VMEM((seconds, rows, wide), dtype),
        pltpu.SemaphoreType.DMA((4,)),
    ]


class Gather:
    def __init__(self, buf, sems, direct=False):
        self.buf, self.sems, self.direct = buf, sems, direct

    def _send(self, device, block, sem):
        block = self.buf.at[block]
        remote_copy("kv", device, block, block, self.sems.at[0], self.sems.at[sem]).start()

    def _across(self, far):
        outer_at, inner_at, outer, inner = place()
        block = (outer_at + outer - far) % outer * inner + inner_at
        for step in range(1, inner):
            self._send(inner_peer(step)[1], block, 2)

    def send(self):
        outer_at, inner_at, outer, inner = place()
        own = lax.axis_index("kv")
        for step in range(outer - 1, 0, -1):
            if self.direct:
                for side in range(1, inner):
                    self._send((outer_at + step) % outer * inner + (inner_at + side) % inner, own, 2)
            self._send(outer_peer(step)[1], own, 1)
        self._across(0)

    def relay(self):
        outer = place()[2]
        wait_bytes(self.buf.at[pl.ds(1, outer - 1)], self.sems.at[1])
        if not self.direct:
            for far in range(1, outer):
                self._across(far)

    def wait(self):
        _, _, outer, inner = place()
        if inner > 1:
            wait_bytes(self.buf.at[pl.ds(0, outer * (inner - 1))], self.sems.at[2])

    def settle(self):
        wait_bytes(self.buf.at[pl.ds(1, self.buf.shape[0] - 1)], self.sems.at[0])


def gather_scratch(count, rows, wide):
    return [pltpu.VMEM((count, rows, wide), BF16), pltpu.SemaphoreType.DMA((3,))]


def tp_send(buf, sems):
    tp = lax.axis_index("tp")
    for step in range(1, buf.shape[0]):
        remote_copy("tp", peer_of("tp", step), buf.at[tp], buf.at[tp], sems.at[0], sems.at[1]).start()


def tp_total(buf, sems):
    wait_bytes(buf.at[pl.ds(1, buf.shape[0] - 1)], sems.at[1])
    total = buf[0].astype(F32)
    for i in range(1, buf.shape[0]):
        total += buf[i].astype(F32)
    return total


def tp_settle(buf, sems):
    wait_bytes(buf.at[pl.ds(1, buf.shape[0] - 1)], sems.at[0])


class Queue:
    def __init__(self, scatters, turn, window, hand):
        self.scatters, self.turn, self.window, self.hand = scatters, turn, window, max(len(scatters) - hand, 0)
        self.tp = lax.axis_index("tp")
        self.paired = lax.axis_size("tp") % 2 == 0

    def _issue(self, k):
        if k >= self.window:
            self.scatters[k - self.window].drain()
        self.scatters[k].start()

    def early(self, k):
        if not self.paired:
            self._issue(k)
            return

        @pl.when(self.tp % 2 == 0)
        def _():
            self._issue(k)
            if k == self.hand:
                pl.semaphore_signal(self.turn, inc=1, device_id={"tp": self.tp + 1}, device_id_type=MESH)

    def late(self):
        if not self.paired:
            return

        @pl.when(self.tp % 2 == 1)
        def _():
            pl.semaphore_wait(self.turn, 1)
            for k in range(len(self.scatters)):
                self._issue(k)

    def finish(self):
        for scatter in self.scatters[-self.window :]:
            scatter.drain()


def padded(wide):
    return -(-wide // LANES) * LANES


def hidden_spans(hidden):
    sizes = []
    while hidden - sum(sizes) >= SPAN + EDGE:
        sizes.append(OUTER_SPAN if len(sizes) in OUTER_AT else SPAN)
    while hidden > sum(sizes):
        sizes.append(min(EDGE, hidden - sum(sizes)))
    return [(sum(sizes[:k]), wide, k not in OUTER_AT) for k, wide in enumerate(sizes)]


def ffn_order(spans):
    hidden = spans[-1][0] + spans[-1][1]
    inner_sum = outer_sum = 0.0
    events = []
    for k, (at, wide, inner_first) in enumerate(spans):
        if inner_first:
            inner_sum += 4.0 * wide / hidden
            second = 0.6 + inner_sum + 2.6
            total = second + 4.2 + 4.0 * wide / hidden
        else:
            outer_sum += 16.0 * wide / hidden
            second = 1.0 + outer_sum + 4.2
            total = second + 2.6 + 4.0 * wide / hidden
        relay = total + 4.0 + 2.0 * wide / hidden
        events += [(at / hidden, 0, k), (second, 1, k), (total, 2, k), (relay, 3, k), (relay + 3.0, 4, k)]
    return [(kind, k) for _, kind, k in sorted(events)]


def layer_kernel(heads, spans, *refs):
    (
        tok_hbm, gain1_hbm, wq, wk, wv, wo, wg, bias_hbm, m_hbm, n_hbm, c_hbm, wout, gain2_hbm, wgf, wuf, wdf,
        mixed_ref, newc_ref, newn_ref, newm_ref,
    ) = refs[:20]
    scratch = list(refs[20:])

    def take(n):
        got = scratch[:n]
        del scratch[:n]
        return got

    tok_v, gain1_v, wq_v, wk_v, wv_v, wo_v, wg_v, wout_v, wgf_v, wuf_v, wdf_v = take(11)
    bias_ref, m_ref, n_ref, gain2_ref, clow = take(5)
    wload, cload, sload = take(3)
    gates_rs = Scatter(*take(5))
    proj_rs = [Scatter(*take(5), i < 1 + 2 * heads) for i in range(2 + 2 * heads)]
    head_ag = [Gather(*take(2), True) for _ in range(heads)]
    ffn_rs = [Scatter(*take(5), span[2]) for span in spans]
    square_rs = Scatter(*take(5))
    ffn_ag = [Gather(*take(2)) for _ in spans]
    abuf, dbuf, mid_v, acc_v, cols_v, asem, dsem, turn = take(8)

    kv = lax.axis_index("kv")
    tp = lax.axis_index("tp")
    count = lax.axis_size("kv")
    outer_at, inner_at, outer, inner = place()
    batch, width = tok_v.shape
    rows = batch // count
    _, _, value_size, query_size = newc_ref.shape
    heads_all = bias_ref.shape[1]
    gate_cols = wg_v.shape[0]

    barrier = pltpu.get_barrier_semaphore()
    signal_peers(barrier, "kv")
    signal_peers(barrier, "tp")
    chunks = [(wq, wq_v, 0, heads * query_size), (wk, wk_v, 0, heads * query_size)]
    for h in range(heads):
        chunks.append((wv, wv_v, h * value_size, value_size))
        chunks.append((wo, wo_v, h * value_size, value_size))
    early = [
        pltpu.make_async_copy(tok_hbm, tok_v, wload.at[0]),
        pltpu.make_async_copy(gain1_hbm, gain1_v, wload.at[1]),
        pltpu.make_async_copy(
            wg.at[:, pl.ds(pl.multiple_of(kv * width, LANES), width)], wg_v, wload.at[2]
        ),
    ]
    for load in early:
        load.start()
    small = [
        pltpu.make_async_copy(src, dst, sload.at[i])
        for i, (src, dst) in enumerate(
            [(bias_hbm, bias_ref), (m_hbm, m_ref), (n_hbm, n_ref), (gain2_hbm, gain2_ref)]
        )
    ]
    for load in small:
        load.start()
    loads = {}
    for i in [0, len(chunks) - 1, *range(1, len(chunks) - 1)]:
        src, dst, at, wide = chunks[i]
        load = pltpu.make_async_copy(
            src.at[:, pl.ds(at, wide)], dst.at[:, pl.ds(at, wide)], wload.at[7 + i]
        )
        load.start()
        loads[i] = load
    early[0].wait()
    early[1].wait()
    tok = tok_v[...].astype(F32)
    normed = (tok * gain1_v[...]).astype(BF16)
    proj_queue = Queue([proj_rs[0], gates_rs, *proj_rs[1:-1]], turn.at[0], PROJ_WINDOW, PROJ_HAND)
    last = len(chunks) - 1
    turns = [0, last, *range(1, last)]
    for i in turns:
        _, dst, at, wide = chunks[i]
        loads[i].wait()
        if i == turns[-1]:
            for h in range(heads):
                for b in range(rows):
                    pltpu.make_async_copy(c_hbm.at[b, h], newc_ref.at[b, h], cload).start()
            late = [
                pltpu.make_async_copy(src, dst, wload.at[3 + i])
                for i, (src, dst) in enumerate([(wout, wout_v), (wgf, wgf_v), (wuf, wuf_v), (wdf, wdf_v)])
            ]
            for load in late:
                load.start()
        out = jnp.dot(normed, dst[:, at : at + wide], preferred_element_type=F32)
        proj_rs[i].put(out, 0, wide)
        if i == 0:
            pl.semaphore_wait(barrier, count - 1 + lax.axis_size("tp") - 1)
            proj_queue.early(0)
            early[2].wait()
            gates = lax.dot_general(
                normed, wg_v[...], (((1,), (1,)), ((), ())), preferred_element_type=F32
            )
            squares = jnp.sum(tok * tok, axis=1, keepdims=True)
            gates_rs.put(jnp.broadcast_to(squares, (batch, LANES)), 0, LANES)
            gates_rs.put(gates, 0, gate_cols)
            proj_queue.early(1)
        elif i == last:
            proj_rs[i].start()
        else:
            proj_queue.early(i + 1)
    proj_queue.late()
    for load in small:
        load.wait()
    proj_rs[0].second()
    gates_rs.second()
    for rs in proj_rs[1:]:
        rs.second()

    wait_bytes(newc_ref, cload)
    for h in range(heads):
        for b in range(rows):
            clow[b, h] = newc_ref[b, h].astype(BF16)
    scale_query = proj_rs[0].total()
    gate_sum = gates_rs.total()
    scale = lax.rsqrt(gate_sum[:, gate_cols : gate_cols + 1] / (width * count) + norm_floor)
    gates = gate_sum * scale
    query_all = scale_query * (scale * query_size ** (-0.5))
    query_low = query_all.astype(BF16)
    lane = lax.broadcasted_iota(jnp.int32, gates.shape, 1)
    bias_lane = lax.broadcasted_iota(jnp.int32, bias_ref.shape, 1)
    sub = lax.broadcasted_iota(jnp.int32, (rows, value_size), 0)
    eye = lax.broadcasted_iota(jnp.int32, (rows, rows), 0) == lax.broadcasted_iota(
        jnp.int32, (rows, rows), 1
    )
    keeps, admits, new_ms = [], [], []
    for h in range(heads):
        column = tp * heads + h
        log_input = jnp.sum(jnp.where(lane == column, gates, 0.0), axis=1, keepdims=True)
        forget = jnp.sum(jnp.where(lane == heads_all + column, gates, 0.0), axis=1, keepdims=True)
        bias = jnp.sum(jnp.where(bias_lane == column, bias_ref[...], 0.0), axis=1, keepdims=True)
        pre = forget + bias
        log_forget = jnp.minimum(pre, 0.0) - jnp.log(1.0 + jnp.exp(-jnp.abs(pre)))
        old_m = jnp.sum(jnp.where(eye, m_ref[h : h + 1, :], 0.0), axis=1, keepdims=True)
        carried = log_forget + old_m
        new_m = jnp.maximum(carried, log_input)
        keeps.append(jnp.exp(carried - new_m))
        admits.append(jnp.exp(log_input - new_m))
        new_ms.append(new_m)
        newm_ref[h : h + 1, :] = jnp.sum(jnp.where(eye, new_m, 0.0), axis=0, keepdims=True)
    reads = []
    for h in range(heads):
        read = jnp.zeros((rows, value_size), F32)
        low = query_low[:, h * query_size : (h + 1) * query_size]
        for b in range(rows):
            one = lax.dot_general(
                low, clow[b, h], (((1,), (1,)), ((), ())), preferred_element_type=F32
            )
            read = jnp.where(sub == b, one, read)
        reads.append(read)
    key_all = proj_rs[1].total() * scale
    keys = []
    for h in range(heads):
        query = query_all[:, h * query_size : (h + 1) * query_size]
        key = admits[h] * key_all[:, h * query_size : (h + 1) * query_size]
        keys.append(key)
        new_n = keeps[h] * n_ref[:, h, :] + key
        newn_ref[:, h, :] = new_n
        denom = jnp.maximum(
            jnp.abs(jnp.sum(new_n * query, axis=1, keepdims=True)), jnp.exp(-new_ms[h])
        )
        value = proj_rs[2 + 2 * h].total() * scale
        numer = keeps[h] * reads[h] + value * jnp.sum(key * query, axis=1, keepdims=True)
        cols_v[h] = value.T
        out_pre = proj_rs[3 + 2 * h].total() * scale
        gated = numer / ((1.0 + jnp.exp(-out_pre)) * denom)
        head_ag[h].buf[kv] = gated.astype(BF16)
        head_ag[h].send()
    for h in range(heads):
        keep_wide = jnp.broadcast_to(keeps[h], (rows, query_size))
        for b in range(rows):
            newc_ref[b, h] = (
                keep_wide[b : b + 1, :] * newc_ref[b, h] + cols_v[h, :, b : b + 1] * keys[h][b : b + 1, :]
            )
        if h == 0:
            for ag in head_ag:
                ag.relay()

    late[0].wait()
    attn = None
    for h in range(heads):
        head_ag[h].wait()
        block = head_ag[h].buf[...].astype(F32).reshape(batch, value_size).astype(BF16)
        one = jnp.dot(block, wout_v[h * value_size : (h + 1) * value_size, :], preferred_element_type=F32)
        attn = one if attn is None else attn + one
    abuf[tp] = attn.astype(BF16)
    tp_send(abuf, asem)
    for group in [gates_rs, *proj_rs, *head_ag]:
        group.settle()
    proj_queue.finish()
    proj_rs[-1].drain()
    attn_mix = tp_total(abuf, asem)
    middle = (tok_v[...].astype(F32) + attn_mix).astype(BF16)
    mid_v[...] = middle
    mid = middle.astype(F32)
    squares = jnp.sum(mid * mid, axis=1, keepdims=True)
    normed = (mid * gain2_ref[...]).astype(BF16)
    square_rs.put(jnp.broadcast_to(squares, (batch, LANES)), 0, LANES)
    late[1].wait()
    late[2].wait()
    ffn_queue = Queue([square_rs, *[rs for rs in ffn_rs if rs.inner_first]], turn.at[1], FFN_WINDOW, FFN_HAND)
    scale2 = None
    for kind, k in ffn_order(spans):
        at, wide, inner_first = spans[k]
        half = padded(wide)
        if kind == 0:
            for j, weight in enumerate([wgf_v, wuf_v]):
                out = lax.dot_general(
                    normed, weight[at : at + wide, :], (((1,), (1,)), ((), ())), preferred_element_type=F32
                )
                ffn_rs[k].put(out, j * half, wide)
                if half > wide:
                    fill = jnp.zeros((batch, half - wide), F32)
                    ffn_rs[k].put(fill, j * half + wide, half - wide)
            if k == 0:
                ffn_queue.early(0)
            if inner_first:
                ffn_queue.early(ffn_queue.scatters.index(ffn_rs[k]))
            else:
                ffn_rs[k].start()
            if k == len(spans) - 1:
                ffn_queue.late()
        elif kind == 1:
            ffn_rs[k].second()
            if k == 0:
                square_rs.second()
        elif kind == 2:
            if scale2 is None:
                total = square_rs.total()
                scale2 = lax.rsqrt(total[:, :1] / (width * count) + norm_floor)
            both = ffn_rs[k].total() * scale2
            gate = both[:, :wide]
            up = both[:, half : half + wide]
            hid = gate / (1.0 + jnp.exp(-gate)) * up
            ffn_ag[k].buf[kv] = hid.astype(BF16)
            ffn_ag[k].send()
        elif kind == 3:
            ffn_ag[k].relay()
        else:
            ffn_ag[k].wait()
            if k == 0:
                late[3].wait()
            hid = ffn_ag[k].buf[...].astype(F32).reshape(batch, wide).astype(BF16)
            one = jnp.dot(hid, wdf_v[at : at + wide, :], preferred_element_type=F32)
            if k == 0:
                acc_v[...] = one
            else:
                acc_v[...] += one
    dbuf[tp] = acc_v[...].astype(BF16)
    tp_send(dbuf, dsem)
    for group in [square_rs, *ffn_rs, *ffn_ag]:
        group.settle()
    ffn_queue.finish()
    for rs in ffn_rs:
        if not rs.inner_first:
            rs.drain()
    tp_settle(abuf, asem)
    down = tp_total(dbuf, dsem)
    mixed_ref[...] = (mid_v[...].astype(F32) + down).astype(BF16)
    tp_settle(dbuf, dsem)


def store_kernel(mixed_in, c_in, n_in, m_in, mixed_out, c_out, n_out, m_out, sems):
    rows = c_in.shape[0]
    copies = [pltpu.make_async_copy(c_in.at[b], c_out.at[b], sems.at[b]) for b in range(rows)]
    copies += [
        pltpu.make_async_copy(src, dst, sems.at[rows + i])
        for i, (src, dst) in enumerate([(mixed_in, mixed_out), (n_in, n_out), (m_in, m_out)])
    ]
    for copy in copies:
        copy.start()
    for copy in copies:
        copy.wait()


def per_device(
    tokens,
    attn_gain,
    w_query,
    w_key,
    w_value,
    w_outgate,
    w_gates,
    forget_bias,
    state_c,
    state_n,
    state_m,
    w_output,
    mlp_gain,
    w_gateff,
    w_upff,
    w_downff,
):
    count = lax.axis_size("kv")
    tps = lax.axis_size("tp")
    batch, width = tokens.shape
    rows, heads, value_size, query_size = state_c.shape
    hidden = w_gateff.shape[1]
    inner = inner_size(count)
    outer = count // inner
    spans = hidden_spans(hidden)
    sem = pltpu.SemaphoreType.DMA
    struct = jax.ShapeDtypeStruct
    args = (
        tokens, attn_gain[None], w_query, w_key, w_value, w_outgate, w_gates.T,
        forget_bias[None], state_m.T, state_n, state_c, w_output, mlp_gain[None],
        w_gateff.T, w_upff.T, w_downff,
    )
    chunks = [heads * query_size] * 2 + [value_size] * (2 * heads)
    scratch = [
        pltpu.VMEM(tokens.shape, BF16),
        pltpu.VMEM((1, width), F32),
        *[pltpu.VMEM(w.shape, BF16) for w in (w_query, w_key, w_value, w_outgate)],
        pltpu.VMEM((w_gates.shape[1], width), BF16),
        *[pltpu.VMEM(w.shape, BF16) for w in (w_output, w_gateff.T, w_upff.T, w_downff)],
        *[pltpu.VMEM(args[i].shape, F32) for i in (7, 8, 9, 12)],
        pltpu.VMEM(state_c.shape, BF16),
        sem((7 + len(chunks),)),
        sem,
        sem((4,)),
    ]
    scratch += scatter_scratch(inner, outer, rows, LANES, F32)
    for wide in chunks[:-1]:
        scratch += scatter_scratch(inner, outer, rows, wide, BF16)
    scratch += scatter_scratch(outer, inner, rows, chunks[-1], BF16)
    for _ in range(heads):
        scratch += gather_scratch(count, rows, value_size)
    for _, wide, inner_first in spans:
        firsts, seconds = (inner, outer) if inner_first else (outer, inner)
        scratch += scatter_scratch(firsts, seconds, rows, 2 * padded(wide), BF16)
    scratch += scatter_scratch(inner, outer, rows, LANES, F32)
    for _, wide, _ in spans:
        scratch += gather_scratch(count, rows, wide)
    scratch += [
        pltpu.VMEM((tps, batch, width), BF16),
        pltpu.VMEM((tps, batch, width), BF16),
        pltpu.VMEM((batch, width), BF16),
        pltpu.VMEM((batch, width), F32),
        pltpu.VMEM((heads, value_size, rows), F32),
        *[sem((2,))] * 2,
        pltpu.SemaphoreType.REGULAR((2,)),
    ]

    def kernel(*refs):
        layer_kernel(heads, spans, *refs)

    kernel_outs = (
        struct((batch, width), BF16),
        struct(state_c.shape, F32),
        struct(state_n.shape, F32),
        struct(state_m.T.shape, F32),
    )
    state_bytes = state_c.size * 4
    outs = pl.pallas_call(
        kernel,
        out_shape=kernel_outs,
        in_specs=[HBM_SPEC] * len(args),
        out_specs=(VMEM_SPEC,) * 4,
        scratch_shapes=scratch,
        compiler_params=pltpu.CompilerParams(
            collective_id=0, has_side_effects=True,
            vmem_limit_bytes=VMEM_ALL - 3 * state_bytes,
        ),
        name="layer",
    )(*[pltpu.with_memory_space_constraint(arg, pltpu.HBM) for arg in args])
    mixed, new_c, new_n, new_m = pl.pallas_call(
        store_kernel,
        out_shape=kernel_outs,
        in_specs=[VMEM_SPEC] * 4,
        out_specs=(HBM_SPEC,) * 4,
        scratch_shapes=[sem((rows + 3,))],
        compiler_params=pltpu.CompilerParams(vmem_limit_bytes=ROOM),
        name="store",
    )(*outs)
    return (mixed, new_c, new_n, new_m.T)


def solution(mesh):
    placed = (
        P(None, "kv"),
        P("kv"),
        P("kv", "tp"),
        P("kv", "tp"),
        P("kv", "tp"),
        P("kv", "tp"),
        P(),
        P(),
        P("kv", "tp", None, None),
        P("kv", "tp", None),
        P("kv", "tp"),
        P("tp", "kv"),
        P("kv"),
        P("kv", "tp"),
        P("kv", "tp"),
        P("tp", "kv"),
    )
    return jax.shard_map(
        per_device,
        mesh=mesh,
        in_specs=placed,
        out_specs=(P(None, "kv"), P("kv", "tp", None, None), P("kv", "tp", None), P("kv", "tp")),
        check_vma=False,
    )
```

```python
import jax
import jax.numpy as jnp
from jax import lax
from jax.experimental import pallas as pl
from jax.experimental.pallas import tpu as pltpu
from jax.sharding import PartitionSpec as P

norm_floor = 1e-05
MESH = pl.DeviceIdType.MESH
LANES = 128
PROJ_WINDOW, PROJ_HAND = 6, 4
FFN_WINDOW, FFN_HAND = 3, 1
SPANS, OUTER_AT = (512, 640, 512, 512, 256), (1,)

VMEM_ALL = 67043328
ROOM = 4 * 1024 * 1024
VMEM_SPEC = pl.BlockSpec(memory_space=pltpu.VMEM)
HBM_SPEC = pl.BlockSpec(memory_space=pltpu.HBM)
F32, BF16 = jnp.float32, jnp.bfloat16


def peer_of(axis, step):
    count = lax.axis_size(axis)
    return lax.rem(lax.axis_index(axis) + step, count)


def signal_peers(barrier, axis):
    for step in range(1, lax.axis_size(axis)):
        pl.semaphore_signal(
            barrier, inc=1, device_id={axis: peer_of(axis, step)}, device_id_type=MESH
        )


def inner_size(count):
    size = 1 << ((count.bit_length() - 1) // 2)
    return size if count % size == 0 else 1


def place():
    count = lax.axis_size("kv")
    inner = inner_size(count)
    kv = lax.axis_index("kv")
    return kv // inner, kv % inner, count // inner, inner


def inner_peer(step):
    outer_at, inner_at, _, inner = place()
    return (inner_at + step) % inner, outer_at * inner + (inner_at + step) % inner


def outer_peer(step):
    outer_at, inner_at, outer, inner = place()
    return (outer_at + step) % outer, ((outer_at + step) % outer) * inner + inner_at


def remote_copy(axis, device, src, dst, send_sem, recv_sem):
    return pltpu.make_async_remote_copy(
        src_ref=src,
        dst_ref=dst,
        send_sem=send_sem,
        recv_sem=recv_sem,
        device_id={axis: device},
        device_id_type=MESH,
    )


def wait_bytes(ref, sem):
    pltpu.make_async_copy(ref, ref, sem).wait()


class Scatter:
    def __init__(self, part, land, both, last, sems, inner_first=True):
        self.part, self.land, self.both, self.last = part, land, both, last
        self.sems, self.inner_first = sems, inner_first
        self.firsts, self.seconds = part.shape[0], part.shape[1]

    def _peers(self):
        return (inner_peer, outer_peer) if self.inner_first else (outer_peer, inner_peer)

    def _places(self):
        outer_at, inner_at, _, _ = place()
        return (inner_at, outer_at) if self.inner_first else (outer_at, inner_at)

    def put(self, out, at, size):
        inner, outer = (self.firsts, self.seconds) if self.inner_first else (self.seconds, self.firsts)
        split = out.reshape(outer, inner, self.part.shape[2], size).astype(self.part.dtype)
        for i in range(self.firsts):
            self.part[i, :, :, at : at + size] = split[:, i] if self.inner_first else split[i]

    def start(self):
        for step in range(self.firsts - 1, 0, -1):
            at, device = self._peers()[0](step)
            remote_copy(
                "kv", device, self.part.at[at], self.land.at[step], self.sems.at[0], self.sems.at[1]
            ).start()

    def drain(self):
        if self.firsts > 1:
            wait_bytes(self.land.at[pl.ds(1, self.firsts - 1)], self.sems.at[0])

    def second(self):
        if self.firsts > 1:
            wait_bytes(self.land.at[pl.ds(1, self.firsts - 1)], self.sems.at[1])
        acc = self.part[self._places()[0]].astype(F32)
        for step in range(1, self.firsts):
            acc += self.land[step].astype(F32)
        self.both[...] = acc.astype(self.both.dtype)
        for step in range(1, self.seconds):
            to, device = self._peers()[1](step)
            remote_copy(
                "kv", device, self.both.at[to], self.last.at[step], self.sems.at[2], self.sems.at[3]
            ).start()

    def total(self):
        if self.seconds > 1:
            wait_bytes(self.last.at[pl.ds(1, self.seconds - 1)], self.sems.at[3])
        acc = self.both[self._places()[1]].astype(F32)
        for step in range(1, self.seconds):
            acc += self.last[step].astype(F32)
        return acc

    def settle(self):
        if self.seconds > 1:
            wait_bytes(self.last.at[pl.ds(1, self.seconds - 1)], self.sems.at[2])


def scatter_scratch(firsts, seconds, rows, wide, dtype):
    return [
        pltpu.VMEM((firsts, seconds, rows, wide), dtype),
        pltpu.VMEM((firsts, seconds, rows, wide), dtype),
        pltpu.VMEM((seconds, rows, wide), dtype),
        pltpu.VMEM((seconds, rows, wide), dtype),
        pltpu.SemaphoreType.DMA((4,)),
    ]


class Gather:
    def __init__(self, buf, sems, direct=False):
        self.buf, self.sems, self.direct = buf, sems, direct

    def _send(self, device, block, sem):
        block = self.buf.at[block]
        remote_copy("kv", device, block, block, self.sems.at[0], self.sems.at[sem]).start()

    def _across(self, far):
        outer_at, inner_at, outer, inner = place()
        block = (outer_at + outer - far) % outer * inner + inner_at
        for step in range(1, inner):
            self._send(inner_peer(step)[1], block, 2)

    def send(self):
        outer_at, inner_at, outer, inner = place()
        own = lax.axis_index("kv")
        for step in range(outer - 1, 0, -1):
            if self.direct:
                for side in range(1, inner):
                    self._send((outer_at + step) % outer * inner + (inner_at + side) % inner, own, 2)
            self._send(outer_peer(step)[1], own, 1)
        self._across(0)

    def relay(self):
        outer = place()[2]
        wait_bytes(self.buf.at[pl.ds(1, outer - 1)], self.sems.at[1])
        if not self.direct:
            for far in range(1, outer):
                self._across(far)

    def wait(self):
        _, _, outer, inner = place()
        if inner > 1:
            wait_bytes(self.buf.at[pl.ds(0, outer * (inner - 1))], self.sems.at[2])

    def settle(self):
        wait_bytes(self.buf.at[pl.ds(1, self.buf.shape[0] - 1)], self.sems.at[0])


def gather_scratch(count, rows, wide):
    return [pltpu.VMEM((count, rows, wide), BF16), pltpu.SemaphoreType.DMA((3,))]


def tp_send(buf, sems):
    tp = lax.axis_index("tp")
    for step in range(1, buf.shape[0]):
        remote_copy("tp", peer_of("tp", step), buf.at[tp], buf.at[tp], sems.at[0], sems.at[1]).start()


def tp_total(buf, sems):
    wait_bytes(buf.at[pl.ds(1, buf.shape[0] - 1)], sems.at[1])
    total = buf[0].astype(F32)
    for i in range(1, buf.shape[0]):
        total += buf[i].astype(F32)
    return total


def tp_settle(buf, sems):
    wait_bytes(buf.at[pl.ds(1, buf.shape[0] - 1)], sems.at[0])


class Queue:
    def __init__(self, scatters, turn, window, hand):
        self.scatters, self.turn, self.window, self.hand = scatters, turn, window, max(len(scatters) - hand, 0)
        self.tp = lax.axis_index("tp")
        self.paired = lax.axis_size("tp") % 2 == 0

    def _issue(self, k):
        if k >= self.window:
            self.scatters[k - self.window].drain()
        self.scatters[k].start()

    def early(self, k):
        if not self.paired:
            self._issue(k)
            return

        @pl.when(self.tp % 2 == 0)
        def _():
            self._issue(k)
            if k == self.hand:
                pl.semaphore_signal(self.turn, inc=1, device_id={"tp": self.tp + 1}, device_id_type=MESH)

    def late(self):
        if not self.paired:
            return

        @pl.when(self.tp % 2 == 1)
        def _():
            pl.semaphore_wait(self.turn, 1)
            for k in range(len(self.scatters)):
                self._issue(k)

    def finish(self):
        for scatter in self.scatters[-self.window :]:
            scatter.drain()


def padded(wide):
    return -(-wide // LANES) * LANES


def hidden_spans(hidden):
    sizes = []
    for wide in SPANS:
        if hidden - sum(sizes) > wide:
            sizes.append(wide)
    while hidden > sum(sizes):
        sizes.append(min(SPANS[-1], hidden - sum(sizes)))
    return [(sum(sizes[:k]), wide, k not in OUTER_AT) for k, wide in enumerate(sizes)]


def ffn_order(spans):
    hidden = spans[-1][0] + spans[-1][1]
    inner_sum = outer_sum = 0.0
    events = []
    for k, (at, wide, inner_first) in enumerate(spans):
        if inner_first:
            inner_sum += 4.0 * wide / hidden
            second = 0.6 + inner_sum + 2.6
            total = second + 4.2 + 4.0 * wide / hidden
        else:
            outer_sum += 16.0 * wide / hidden
            second = 1.0 + outer_sum + 4.2
            total = second + 2.6 + 4.0 * wide / hidden
        relay = total + 4.0 + 2.0 * wide / hidden
        events += [(at / hidden, 0, k), (second, 1, k), (total, 2, k), (relay, 3, k), (relay + 3.0, 4, k)]
    return [(kind, k) for _, kind, k in sorted(events)]


def layer_kernel(heads, spans, *refs):
    (
        tok_hbm, gain1_hbm, wq, wk, wv, wo, wg, bias_hbm, m_hbm, n_hbm, c_hbm, wout, gain2_hbm, wgf, wuf, wdf,
        mixed_ref, newc_ref, newn_ref, newm_ref,
    ) = refs[:20]
    scratch = list(refs[20:])

    def take(n):
        got = scratch[:n]
        del scratch[:n]
        return got

    tok_v, gain1_v, wq_v, wk_v, wv_v, wo_v, wg_v, wout_v, wgf_v, wuf_v, wdf_v = take(11)
    bias_ref, m_ref, n_ref, gain2_ref, clow = take(5)
    wload, cload, sload = take(3)
    gates_rs = Scatter(*take(5))
    proj_rs = [Scatter(*take(5), i < 1 + 2 * heads) for i in range(2 + 2 * heads)]
    head_ag = [Gather(*take(2), True) for _ in range(heads)]
    ffn_rs = [Scatter(*take(5), span[2]) for span in spans]
    square_rs = Scatter(*take(5))
    ffn_ag = [Gather(*take(2)) for _ in spans]
    abuf, dbuf, mid_v, acc_v, cols_v, asem, dsem, turn = take(8)

    kv = lax.axis_index("kv")
    tp = lax.axis_index("tp")
    count = lax.axis_size("kv")
    outer_at, inner_at, outer, inner = place()
    batch, width = tok_v.shape
    rows = batch // count
    _, _, value_size, query_size = newc_ref.shape
    heads_all = bias_ref.shape[1]
    gate_cols = wg_v.shape[0]

    barrier = pltpu.get_barrier_semaphore()
    signal_peers(barrier, "kv")
    signal_peers(barrier, "tp")
    chunks = [(wq, wq_v, 0, heads * query_size), (wk, wk_v, 0, heads * query_size)]
    for h in range(heads):
        chunks.append((wv, wv_v, h * value_size, value_size))
        chunks.append((wo, wo_v, h * value_size, value_size))
    early = [
        pltpu.make_async_copy(tok_hbm, tok_v, wload.at[0]),
        pltpu.make_async_copy(gain1_hbm, gain1_v, wload.at[1]),
        pltpu.make_async_copy(
            wg.at[:, pl.ds(pl.multiple_of(kv * width, LANES), width)], wg_v, wload.at[2]
        ),
    ]
    for load in early:
        load.start()
    small = [
        pltpu.make_async_copy(src, dst, sload.at[i])
        for i, (src, dst) in enumerate(
            [(bias_hbm, bias_ref), (m_hbm, m_ref), (n_hbm, n_ref), (gain2_hbm, gain2_ref)]
        )
    ]
    for load in small:
        load.start()
    loads = {}
    for i in [0, 1, len(chunks) - 1, *range(2, len(chunks) - 1)]:
        src, dst, at, wide = chunks[i]
        load = pltpu.make_async_copy(
            src.at[:, pl.ds(at, wide)], dst.at[:, pl.ds(at, wide)], wload.at[7 + i]
        )
        load.start()
        loads[i] = load
    early[0].wait()
    early[1].wait()
    tok = tok_v[...].astype(F32)
    normed = (tok * gain1_v[...]).astype(BF16)
    proj_queue = Queue([proj_rs[0], gates_rs, *proj_rs[1:-1]], turn.at[0], PROJ_WINDOW, PROJ_HAND)
    last = len(chunks) - 1
    turns = [0, 1, last, *range(2, last)]
    for i in turns:
        _, dst, at, wide = chunks[i]
        loads[i].wait()
        if i == turns[-1]:
            for h in range(heads):
                for b in range(rows):
                    pltpu.make_async_copy(c_hbm.at[b, h], newc_ref.at[b, h], cload).start()
            late = [
                pltpu.make_async_copy(src, dst, wload.at[3 + i])
                for i, (src, dst) in enumerate([(wout, wout_v), (wgf, wgf_v), (wuf, wuf_v), (wdf, wdf_v)])
            ]
            for load in late:
                load.start()
        out = jnp.dot(normed, dst[:, at : at + wide], preferred_element_type=F32)
        proj_rs[i].put(out, 0, wide)
        if i == 0:
            pl.semaphore_wait(barrier, count - 1 + lax.axis_size("tp") - 1)
            proj_queue.early(0)
            early[2].wait()
            gates = lax.dot_general(
                normed, wg_v[...], (((1,), (1,)), ((), ())), preferred_element_type=F32
            )
            squares = jnp.sum(tok * tok, axis=1, keepdims=True)
            gates_rs.put(jnp.broadcast_to(squares, (batch, LANES)), 0, LANES)
            gates_rs.put(gates, 0, gate_cols)
            proj_queue.early(1)
        elif i == last:
            proj_rs[i].start()
        else:
            proj_queue.early(i + 1)
    proj_queue.late()
    for load in small:
        load.wait()
    proj_rs[0].second()
    gates_rs.second()
    for rs in proj_rs[1:]:
        rs.second()

    wait_bytes(newc_ref, cload)
    for h in range(heads):
        for b in range(rows):
            clow[b, h] = newc_ref[b, h].astype(BF16)
    scale_query = proj_rs[0].total()
    gate_sum = gates_rs.total()
    scale = lax.rsqrt(gate_sum[:, gate_cols : gate_cols + 1] / (width * count) + norm_floor)
    gates = gate_sum * scale
    query_all = scale_query * (scale * query_size ** (-0.5))
    query_low = query_all.astype(BF16)
    lane = lax.broadcasted_iota(jnp.int32, gates.shape, 1)
    bias_lane = lax.broadcasted_iota(jnp.int32, bias_ref.shape, 1)
    sub = lax.broadcasted_iota(jnp.int32, (rows, value_size), 0)
    eye = lax.broadcasted_iota(jnp.int32, (rows, rows), 0) == lax.broadcasted_iota(
        jnp.int32, (rows, rows), 1
    )
    keeps, admits, new_ms = [], [], []
    for h in range(heads):
        column = tp * heads + h
        log_input = jnp.sum(jnp.where(lane == column, gates, 0.0), axis=1, keepdims=True)
        forget = jnp.sum(jnp.where(lane == heads_all + column, gates, 0.0), axis=1, keepdims=True)
        bias = jnp.sum(jnp.where(bias_lane == column, bias_ref[...], 0.0), axis=1, keepdims=True)
        pre = forget + bias
        log_forget = jnp.minimum(pre, 0.0) - jnp.log(1.0 + jnp.exp(-jnp.abs(pre)))
        old_m = jnp.sum(jnp.where(eye, m_ref[h : h + 1, :], 0.0), axis=1, keepdims=True)
        carried = log_forget + old_m
        new_m = jnp.maximum(carried, log_input)
        keeps.append(jnp.exp(carried - new_m))
        admits.append(jnp.exp(log_input - new_m))
        new_ms.append(new_m)
        newm_ref[h : h + 1, :] = jnp.sum(jnp.where(eye, new_m, 0.0), axis=0, keepdims=True)
    reads = []
    for h in range(heads):
        read = jnp.zeros((rows, value_size), F32)
        low = query_low[:, h * query_size : (h + 1) * query_size]
        for b in range(rows):
            one = lax.dot_general(
                low, clow[b, h], (((1,), (1,)), ((), ())), preferred_element_type=F32
            )
            read = jnp.where(sub == b, one, read)
        reads.append(read)
    key_all = proj_rs[1].total() * scale
    keys = []
    for h in range(heads):
        query = query_all[:, h * query_size : (h + 1) * query_size]
        key = admits[h] * key_all[:, h * query_size : (h + 1) * query_size]
        keys.append(key)
        new_n = keeps[h] * n_ref[:, h, :] + key
        newn_ref[:, h, :] = new_n
        denom = jnp.maximum(
            jnp.abs(jnp.sum(new_n * query, axis=1, keepdims=True)), jnp.exp(-new_ms[h])
        )
        value = proj_rs[2 + 2 * h].total() * scale
        numer = keeps[h] * reads[h] + value * jnp.sum(key * query, axis=1, keepdims=True)
        cols_v[h] = value.T
        out_pre = proj_rs[3 + 2 * h].total() * scale
        gated = numer / ((1.0 + jnp.exp(-out_pre)) * denom)
        head_ag[h].buf[kv] = gated.astype(BF16)
        head_ag[h].send()
    for h in range(heads):
        keep_wide = jnp.broadcast_to(keeps[h], (rows, query_size))
        for b in range(rows):
            newc_ref[b, h] = (
                keep_wide[b : b + 1, :] * newc_ref[b, h] + cols_v[h, :, b : b + 1] * keys[h][b : b + 1, :]
            )
    for ag in head_ag:
        ag.relay()

    late[0].wait()
    attn = None
    for h in range(heads):
        head_ag[h].wait()
        block = head_ag[h].buf[...].astype(F32).reshape(batch, value_size).astype(BF16)
        one = jnp.dot(block, wout_v[h * value_size : (h + 1) * value_size, :], preferred_element_type=F32)
        attn = one if attn is None else attn + one
    abuf[tp] = attn.astype(BF16)
    tp_send(abuf, asem)
    for group in [gates_rs, *proj_rs, *head_ag]:
        group.settle()
    proj_queue.finish()
    proj_rs[-1].drain()
    attn_mix = tp_total(abuf, asem)
    middle = (tok_v[...].astype(F32) + attn_mix).astype(BF16)
    mid_v[...] = middle
    mid = middle.astype(F32)
    squares = jnp.sum(mid * mid, axis=1, keepdims=True)
    normed = (mid * gain2_ref[...]).astype(BF16)
    square_rs.put(jnp.broadcast_to(squares, (batch, LANES)), 0, LANES)
    late[1].wait()
    late[2].wait()
    ffn_queue = Queue([square_rs, *[rs for rs in ffn_rs if rs.inner_first]], turn.at[1], FFN_WINDOW, FFN_HAND)
    scale2 = None
    order = ffn_order(spans)
    seconds = [k for kind, k in order if kind == 1]
    for kind, k in order:
        at, wide, inner_first = spans[k]
        half = padded(wide)
        if kind == 0:
            for j, weight in enumerate([wgf_v, wuf_v]):
                out = lax.dot_general(
                    normed, weight[at : at + wide, :], (((1,), (1,)), ((), ())), preferred_element_type=F32
                )
                ffn_rs[k].put(out, j * half, wide)
                if half > wide:
                    fill = jnp.zeros((batch, half - wide), F32)
                    ffn_rs[k].put(fill, j * half + wide, half - wide)
            if k == 0:
                ffn_queue.early(0)
            if inner_first:
                ffn_queue.early(ffn_queue.scatters.index(ffn_rs[k]))
            else:
                ffn_rs[k].start()
            if k == len(spans) - 1:
                ffn_queue.late()
        elif kind == 1:
            ffn_rs[k].second()
            if k == seconds[0]:
                square_rs.second()
        elif kind == 2:
            if scale2 is None:
                total = square_rs.total()
                scale2 = lax.rsqrt(total[:, :1] / (width * count) + norm_floor)
            both = ffn_rs[k].total() * scale2
            gate = both[:, :wide]
            up = both[:, half : half + wide]
            hid = gate / (1.0 + jnp.exp(-gate)) * up
            ffn_ag[k].buf[kv] = hid.astype(BF16)
            ffn_ag[k].send()
        elif kind == 3:
            ffn_ag[k].relay()
        else:
            ffn_ag[k].wait()
            if k == 0:
                late[3].wait()
            hid = ffn_ag[k].buf[...].astype(F32).reshape(batch, wide).astype(BF16)
            one = jnp.dot(hid, wdf_v[at : at + wide, :], preferred_element_type=F32)
            if k == 0:
                acc_v[...] = one
            else:
                acc_v[...] += one
    dbuf[tp] = acc_v[...].astype(BF16)
    tp_send(dbuf, dsem)
    for group in [square_rs, *ffn_rs, *ffn_ag]:
        group.settle()
    ffn_queue.finish()
    for rs in ffn_rs:
        if not rs.inner_first:
            rs.drain()
    tp_settle(abuf, asem)
    down = tp_total(dbuf, dsem)
    mixed_ref[...] = (mid_v[...].astype(F32) + down).astype(BF16)
    tp_settle(dbuf, dsem)


def store_kernel(mixed_in, c_in, n_in, m_in, mixed_out, c_out, n_out, m_out, sems):
    rows = c_in.shape[0]
    copies = [pltpu.make_async_copy(c_in.at[b], c_out.at[b], sems.at[b]) for b in range(rows)]
    copies += [
        pltpu.make_async_copy(src, dst, sems.at[rows + i])
        for i, (src, dst) in enumerate([(mixed_in, mixed_out), (n_in, n_out), (m_in, m_out)])
    ]
    for copy in copies:
        copy.start()
    for copy in copies:
        copy.wait()


def per_device(
    tokens,
    attn_gain,
    w_query,
    w_key,
    w_value,
    w_outgate,
    w_gates,
    forget_bias,
    state_c,
    state_n,
    state_m,
    w_output,
    mlp_gain,
    w_gateff,
    w_upff,
    w_downff,
):
    count = lax.axis_size("kv")
    tps = lax.axis_size("tp")
    batch, width = tokens.shape
    rows, heads, value_size, query_size = state_c.shape
    hidden = w_gateff.shape[1]
    inner = inner_size(count)
    outer = count // inner
    spans = hidden_spans(hidden)
    sem = pltpu.SemaphoreType.DMA
    struct = jax.ShapeDtypeStruct
    args = (
        tokens, attn_gain[None], w_query, w_key, w_value, w_outgate, w_gates.T,
        forget_bias[None], state_m.T, state_n, state_c, w_output, mlp_gain[None],
        w_gateff.T, w_upff.T, w_downff,
    )
    chunks = [heads * query_size] * 2 + [value_size] * (2 * heads)
    scratch = [
        pltpu.VMEM(tokens.shape, BF16),
        pltpu.VMEM((1, width), F32),
        *[pltpu.VMEM(w.shape, BF16) for w in (w_query, w_key, w_value, w_outgate)],
        pltpu.VMEM((w_gates.shape[1], width), BF16),
        *[pltpu.VMEM(w.shape, BF16) for w in (w_output, w_gateff.T, w_upff.T, w_downff)],
        *[pltpu.VMEM(args[i].shape, F32) for i in (7, 8, 9, 12)],
        pltpu.VMEM(state_c.shape, BF16),
        sem((7 + len(chunks),)),
        sem,
        sem((4,)),
    ]
    scratch += scatter_scratch(inner, outer, rows, LANES, F32)
    for wide in chunks[:-1]:
        scratch += scatter_scratch(inner, outer, rows, wide, BF16)
    scratch += scatter_scratch(outer, inner, rows, chunks[-1], BF16)
    for _ in range(heads):
        scratch += gather_scratch(count, rows, value_size)
    for _, wide, inner_first in spans:
        firsts, seconds = (inner, outer) if inner_first else (outer, inner)
        scratch += scatter_scratch(firsts, seconds, rows, 2 * padded(wide), BF16)
    scratch += scatter_scratch(inner, outer, rows, LANES, F32)
    for _, wide, _ in spans:
        scratch += gather_scratch(count, rows, wide)
    scratch += [
        pltpu.VMEM((tps, batch, width), BF16),
        pltpu.VMEM((tps, batch, width), BF16),
        pltpu.VMEM((batch, width), BF16),
        pltpu.VMEM((batch, width), F32),
        pltpu.VMEM((heads, value_size, rows), F32),
        *[sem((2,))] * 2,
        pltpu.SemaphoreType.REGULAR((2,)),
    ]

    def kernel(*refs):
        layer_kernel(heads, spans, *refs)

    kernel_outs = (
        struct((batch, width), BF16),
        struct(state_c.shape, F32),
        struct(state_n.shape, F32),
        struct(state_m.T.shape, F32),
    )
    state_bytes = state_c.size * 4
    outs = pl.pallas_call(
        kernel,
        out_shape=kernel_outs,
        in_specs=[HBM_SPEC] * len(args),
        out_specs=(VMEM_SPEC,) * 4,
        scratch_shapes=scratch,
        compiler_params=pltpu.CompilerParams(
            collective_id=0, has_side_effects=True,
            vmem_limit_bytes=VMEM_ALL - 3 * state_bytes,
        ),
        name="layer",
    )(*[pltpu.with_memory_space_constraint(arg, pltpu.HBM) for arg in args])
    mixed, new_c, new_n, new_m = pl.pallas_call(
        store_kernel,
        out_shape=kernel_outs,
        in_specs=[VMEM_SPEC] * 4,
        out_specs=(HBM_SPEC,) * 4,
        scratch_shapes=[sem((rows + 3,))],
        compiler_params=pltpu.CompilerParams(vmem_limit_bytes=ROOM),
        name="store",
    )(*outs)
    return (mixed, new_c, new_n, new_m.T)


def solution(mesh):
    placed = (
        P(None, "kv"),
        P("kv"),
        P("kv", "tp"),
        P("kv", "tp"),
        P("kv", "tp"),
        P("kv", "tp"),
        P(),
        P(),
        P("kv", "tp", None, None),
        P("kv", "tp", None),
        P("kv", "tp"),
        P("tp", "kv"),
        P("kv"),
        P("kv", "tp"),
        P("kv", "tp"),
        P("tp", "kv"),
    )
    return jax.shard_map(
        per_device,
        mesh=mesh,
        in_specs=placed,
        out_specs=(P(None, "kv"), P("kv", "tp", None, None), P("kv", "tp", None), P("kv", "tp")),
        check_vma=False,
    )
```

```python
import jax
import jax.numpy as jnp
from jax import lax
from jax.experimental import pallas as pl
from jax.experimental.pallas import tpu as pltpu
from jax.sharding import PartitionSpec as P

norm_floor = 1e-05
MESH = pl.DeviceIdType.MESH
LANES = 128
PROJ_WINDOW, PROJ_HAND = 6, 4
FFN_WINDOW, FFN_HAND = 3, 1
SPANS, OUTER_AT = (512, 640, 512, 512, 320, 256), (1,)

VMEM_ALL = 67043328
ROOM = 4 * 1024 * 1024
VMEM_SPEC = pl.BlockSpec(memory_space=pltpu.VMEM)
HBM_SPEC = pl.BlockSpec(memory_space=pltpu.HBM)
F32, BF16 = jnp.float32, jnp.bfloat16


def peer_of(axis, step):
    count = lax.axis_size(axis)
    return lax.rem(lax.axis_index(axis) + step, count)


def signal_peers(barrier, axis):
    for step in range(1, lax.axis_size(axis)):
        pl.semaphore_signal(
            barrier, inc=1, device_id={axis: peer_of(axis, step)}, device_id_type=MESH
        )


def inner_size(count):
    size = 1 << ((count.bit_length() - 1) // 2)
    return size if count % size == 0 else 1


def place():
    count = lax.axis_size("kv")
    inner = inner_size(count)
    kv = lax.axis_index("kv")
    return kv // inner, kv % inner, count // inner, inner


def inner_peer(step):
    outer_at, inner_at, _, inner = place()
    return (inner_at + step) % inner, outer_at * inner + (inner_at + step) % inner


def outer_peer(step):
    outer_at, inner_at, outer, inner = place()
    return (outer_at + step) % outer, ((outer_at + step) % outer) * inner + inner_at


def remote_copy(axis, device, src, dst, send_sem, recv_sem):
    return pltpu.make_async_remote_copy(
        src_ref=src,
        dst_ref=dst,
        send_sem=send_sem,
        recv_sem=recv_sem,
        device_id={axis: device},
        device_id_type=MESH,
    )


def wait_bytes(ref, sem):
    pltpu.make_async_copy(ref, ref, sem).wait()


class Scatter:
    def __init__(self, part, land, both, last, sems, inner_first=True):
        self.part, self.land, self.both, self.last = part, land, both, last
        self.sems, self.inner_first = sems, inner_first
        self.firsts, self.seconds = part.shape[0], part.shape[1]

    def _peers(self):
        return (inner_peer, outer_peer) if self.inner_first else (outer_peer, inner_peer)

    def _places(self):
        outer_at, inner_at, _, _ = place()
        return (inner_at, outer_at) if self.inner_first else (outer_at, inner_at)

    def put(self, out, at, size):
        inner, outer = (self.firsts, self.seconds) if self.inner_first else (self.seconds, self.firsts)
        split = out.reshape(outer, inner, self.part.shape[2], size).astype(self.part.dtype)
        for i in range(self.firsts):
            self.part[i, :, :, at : at + size] = split[:, i] if self.inner_first else split[i]

    def start(self):
        for step in range(self.firsts - 1, 0, -1):
            at, device = self._peers()[0](step)
            remote_copy(
                "kv", device, self.part.at[at], self.land.at[step], self.sems.at[0], self.sems.at[1]
            ).start()

    def drain(self):
        if self.firsts > 1:
            wait_bytes(self.land.at[pl.ds(1, self.firsts - 1)], self.sems.at[0])

    def second(self):
        if self.firsts > 1:
            wait_bytes(self.land.at[pl.ds(1, self.firsts - 1)], self.sems.at[1])
        acc = self.part[self._places()[0]].astype(F32)
        for step in range(1, self.firsts):
            acc += self.land[step].astype(F32)
        self.both[...] = acc.astype(self.both.dtype)
        for step in range(1, self.seconds):
            to, device = self._peers()[1](step)
            remote_copy(
                "kv", device, self.both.at[to], self.last.at[step], self.sems.at[2], self.sems.at[3]
            ).start()

    def total(self):
        if self.seconds > 1:
            wait_bytes(self.last.at[pl.ds(1, self.seconds - 1)], self.sems.at[3])
        acc = self.both[self._places()[1]].astype(F32)
        for step in range(1, self.seconds):
            acc += self.last[step].astype(F32)
        return acc

    def settle(self):
        if self.seconds > 1:
            wait_bytes(self.last.at[pl.ds(1, self.seconds - 1)], self.sems.at[2])


def scatter_scratch(firsts, seconds, rows, wide, dtype):
    return [
        pltpu.VMEM((firsts, seconds, rows, wide), dtype),
        pltpu.VMEM((firsts, seconds, rows, wide), dtype),
        pltpu.VMEM((seconds, rows, wide), dtype),
        pltpu.VMEM((seconds, rows, wide), dtype),
        pltpu.SemaphoreType.DMA((4,)),
    ]


class Gather:
    def __init__(self, buf, sems, direct=False):
        self.buf, self.sems, self.direct = buf, sems, direct

    def _send(self, device, block, sem):
        block = self.buf.at[block]
        remote_copy("kv", device, block, block, self.sems.at[0], self.sems.at[sem]).start()

    def _across(self, far):
        outer_at, inner_at, outer, inner = place()
        block = (outer_at + outer - far) % outer * inner + inner_at
        for step in range(1, inner):
            self._send(inner_peer(step)[1], block, 2)

    def send(self):
        outer_at, inner_at, outer, inner = place()
        own = lax.axis_index("kv")
        for step in range(outer - 1, 0, -1):
            if self.direct:
                for side in range(1, inner):
                    self._send((outer_at + step) % outer * inner + (inner_at + side) % inner, own, 2)
            self._send(outer_peer(step)[1], own, 1)
        self._across(0)

    def relay(self):
        outer = place()[2]
        wait_bytes(self.buf.at[pl.ds(1, outer - 1)], self.sems.at[1])
        if not self.direct:
            for far in range(1, outer):
                self._across(far)

    def wait(self):
        _, _, outer, inner = place()
        if inner > 1:
            wait_bytes(self.buf.at[pl.ds(0, outer * (inner - 1))], self.sems.at[2])

    def settle(self):
        wait_bytes(self.buf.at[pl.ds(1, self.buf.shape[0] - 1)], self.sems.at[0])


def gather_scratch(count, rows, wide):
    return [pltpu.VMEM((count, rows, wide), BF16), pltpu.SemaphoreType.DMA((3,))]


def tp_send(buf, sems):
    tp = lax.axis_index("tp")
    for step in range(1, buf.shape[0]):
        remote_copy("tp", peer_of("tp", step), buf.at[tp], buf.at[tp], sems.at[0], sems.at[1]).start()


def tp_total(buf, sems):
    wait_bytes(buf.at[pl.ds(1, buf.shape[0] - 1)], sems.at[1])
    total = buf[0].astype(F32)
    for i in range(1, buf.shape[0]):
        total += buf[i].astype(F32)
    return total


def tp_settle(buf, sems):
    wait_bytes(buf.at[pl.ds(1, buf.shape[0] - 1)], sems.at[0])


class Queue:
    def __init__(self, scatters, turn, window, hand):
        self.scatters, self.turn, self.window, self.hand = scatters, turn, window, max(len(scatters) - hand, 0)
        self.tp = lax.axis_index("tp")
        self.paired = lax.axis_size("tp") % 2 == 0

    def _issue(self, k):
        if k >= self.window:
            self.scatters[k - self.window].drain()
        self.scatters[k].start()

    def early(self, k):
        if not self.paired:
            self._issue(k)
            return

        @pl.when(self.tp % 2 == 0)
        def _():
            self._issue(k)
            if k == self.hand:
                pl.semaphore_signal(self.turn, inc=1, device_id={"tp": self.tp + 1}, device_id_type=MESH)

    def late(self):
        if not self.paired:
            return

        @pl.when(self.tp % 2 == 1)
        def _():
            pl.semaphore_wait(self.turn, 1)
            for k in range(len(self.scatters)):
                self._issue(k)

    def finish(self):
        for scatter in self.scatters[-self.window :]:
            scatter.drain()


def padded(wide):
    return -(-wide // LANES) * LANES


def hidden_spans(hidden):
    sizes = []
    for wide in SPANS:
        if hidden - sum(sizes) > wide:
            sizes.append(wide)
    while hidden > sum(sizes):
        sizes.append(min(SPANS[-1], hidden - sum(sizes)))
    return [(sum(sizes[:k]), wide, k not in OUTER_AT) for k, wide in enumerate(sizes)]


def ffn_order(spans):
    hidden = spans[-1][0] + spans[-1][1]
    inner_sum = outer_sum = 0.0
    events = []
    for k, (at, wide, inner_first) in enumerate(spans):
        if inner_first:
            inner_sum += 4.0 * wide / hidden
            second = 0.6 + inner_sum + 2.6
            total = second + 4.2 + 4.0 * wide / hidden
        else:
            outer_sum += 16.0 * wide / hidden
            second = 1.0 + outer_sum + 4.2
            total = second + 2.6 + 4.0 * wide / hidden
        relay = total + 4.0 + 2.0 * wide / hidden
        events += [(at / hidden, 0, k), (second, 1, k), (total, 2, k), (relay, 3, k), (relay + 3.0, 4, k)]
    return [(kind, k) for _, kind, k in sorted(events)]


def layer_kernel(heads, spans, *refs):
    (
        tok_hbm, gain1_hbm, wq, wk, wv, wo, wg, bias_hbm, m_hbm, n_hbm, c_hbm, wout, gain2_hbm, wgf, wuf, wdf,
        mixed_ref, newc_ref, newn_ref, newm_ref,
    ) = refs[:20]
    scratch = list(refs[20:])

    def take(n):
        got = scratch[:n]
        del scratch[:n]
        return got

    tok_v, gain1_v, wq_v, wk_v, wv_v, wo_v, wg_v, wout_v, wgf_v, wuf_v, wdf_v = take(11)
    bias_ref, m_ref, n_ref, gain2_ref, clow = take(5)
    wload, cload, sload = take(3)
    gates_rs = Scatter(*take(5))
    proj_rs = [Scatter(*take(5), i < 1 + 2 * heads) for i in range(2 + 2 * heads)]
    head_ag = [Gather(*take(2), True) for _ in range(heads)]
    ffn_rs = [Scatter(*take(5), span[2]) for span in spans]
    square_rs = Scatter(*take(5))
    ffn_ag = [Gather(*take(2)) for _ in spans]
    abuf, dbuf, mid_v, acc_v, cols_v, asem, dsem, turn = take(8)

    kv = lax.axis_index("kv")
    tp = lax.axis_index("tp")
    count = lax.axis_size("kv")
    outer_at, inner_at, outer, inner = place()
    batch, width = tok_v.shape
    rows = batch // count
    _, _, value_size, query_size = newc_ref.shape
    heads_all = bias_ref.shape[1]
    gate_cols = wg_v.shape[0]

    barrier = pltpu.get_barrier_semaphore()
    signal_peers(barrier, "kv")
    signal_peers(barrier, "tp")
    chunks = [(wq, wq_v, 0, heads * query_size), (wk, wk_v, 0, heads * query_size)]
    for h in range(heads):
        chunks.append((wv, wv_v, h * value_size, value_size))
        chunks.append((wo, wo_v, h * value_size, value_size))
    early = [
        pltpu.make_async_copy(tok_hbm, tok_v, wload.at[0]),
        pltpu.make_async_copy(gain1_hbm, gain1_v, wload.at[1]),
        pltpu.make_async_copy(
            wg.at[:, pl.ds(pl.multiple_of(kv * width, LANES), width)], wg_v, wload.at[2]
        ),
    ]
    for load in early:
        load.start()
    small = [
        pltpu.make_async_copy(src, dst, sload.at[i])
        for i, (src, dst) in enumerate(
            [(bias_hbm, bias_ref), (m_hbm, m_ref), (n_hbm, n_ref), (gain2_hbm, gain2_ref)]
        )
    ]
    for load in small:
        load.start()
    loads = {}
    for i in [0, 1, len(chunks) - 1, *range(2, len(chunks) - 1)]:
        src, dst, at, wide = chunks[i]
        load = pltpu.make_async_copy(
            src.at[:, pl.ds(at, wide)], dst.at[:, pl.ds(at, wide)], wload.at[7 + i]
        )
        load.start()
        loads[i] = load
    early[0].wait()
    early[1].wait()
    tok = tok_v[...].astype(F32)
    normed = (tok * gain1_v[...]).astype(BF16)
    proj_queue = Queue([proj_rs[0], gates_rs, *proj_rs[1:-1]], turn.at[0], PROJ_WINDOW, PROJ_HAND)
    last = len(chunks) - 1
    turns = [0, 1, last, *range(2, last)]
    for i in turns:
        _, dst, at, wide = chunks[i]
        loads[i].wait()
        if i == turns[-1]:
            for h in range(heads):
                for b in range(rows):
                    pltpu.make_async_copy(c_hbm.at[b, h], newc_ref.at[b, h], cload).start()
            late = [
                pltpu.make_async_copy(src, dst, wload.at[3 + i])
                for i, (src, dst) in enumerate([(wout, wout_v), (wgf, wgf_v), (wuf, wuf_v), (wdf, wdf_v)])
            ]
            for load in late:
                load.start()
        out = jnp.dot(normed, dst[:, at : at + wide], preferred_element_type=F32)
        proj_rs[i].put(out, 0, wide)
        if i == 0:
            pl.semaphore_wait(barrier, count - 1 + lax.axis_size("tp") - 1)
            proj_queue.early(0)
            early[2].wait()
            gates = lax.dot_general(
                normed, wg_v[...], (((1,), (1,)), ((), ())), preferred_element_type=F32
            )
            squares = jnp.sum(tok * tok, axis=1, keepdims=True)
            gates_rs.put(jnp.broadcast_to(squares, (batch, LANES)), 0, LANES)
            gates_rs.put(gates, 0, gate_cols)
            proj_queue.early(1)
        elif i == last:
            proj_rs[i].start()
        else:
            proj_queue.early(i + 1)
    proj_queue.late()
    for load in small:
        load.wait()
    proj_rs[0].second()
    gates_rs.second()
    for rs in proj_rs[1:]:
        rs.second()

    wait_bytes(newc_ref, cload)
    for h in range(heads):
        for b in range(rows):
            clow[b, h] = newc_ref[b, h].astype(BF16)
    scale_query = proj_rs[0].total()
    gate_sum = gates_rs.total()
    scale = lax.rsqrt(gate_sum[:, gate_cols : gate_cols + 1] / (width * count) + norm_floor)
    gates = gate_sum * scale
    query_all = scale_query * (scale * query_size ** (-0.5))
    query_low = query_all.astype(BF16)
    lane = lax.broadcasted_iota(jnp.int32, gates.shape, 1)
    bias_lane = lax.broadcasted_iota(jnp.int32, bias_ref.shape, 1)
    sub = lax.broadcasted_iota(jnp.int32, (rows, value_size), 0)
    eye = lax.broadcasted_iota(jnp.int32, (rows, rows), 0) == lax.broadcasted_iota(
        jnp.int32, (rows, rows), 1
    )
    keeps, admits, new_ms = [], [], []
    for h in range(heads):
        column = tp * heads + h
        log_input = jnp.sum(jnp.where(lane == column, gates, 0.0), axis=1, keepdims=True)
        forget = jnp.sum(jnp.where(lane == heads_all + column, gates, 0.0), axis=1, keepdims=True)
        bias = jnp.sum(jnp.where(bias_lane == column, bias_ref[...], 0.0), axis=1, keepdims=True)
        pre = forget + bias
        log_forget = jnp.minimum(pre, 0.0) - jnp.log(1.0 + jnp.exp(-jnp.abs(pre)))
        old_m = jnp.sum(jnp.where(eye, m_ref[h : h + 1, :], 0.0), axis=1, keepdims=True)
        carried = log_forget + old_m
        new_m = jnp.maximum(carried, log_input)
        keeps.append(jnp.exp(carried - new_m))
        admits.append(jnp.exp(log_input - new_m))
        new_ms.append(new_m)
        newm_ref[h : h + 1, :] = jnp.sum(jnp.where(eye, new_m, 0.0), axis=0, keepdims=True)
    reads = []
    for h in range(heads):
        read = jnp.zeros((rows, value_size), F32)
        low = query_low[:, h * query_size : (h + 1) * query_size]
        for b in range(rows):
            one = lax.dot_general(
                low, clow[b, h], (((1,), (1,)), ((), ())), preferred_element_type=F32
            )
            read = jnp.where(sub == b, one, read)
        reads.append(read)
    key_all = proj_rs[1].total() * scale
    keys = []
    for h in range(heads):
        query = query_all[:, h * query_size : (h + 1) * query_size]
        key = admits[h] * key_all[:, h * query_size : (h + 1) * query_size]
        keys.append(key)
        new_n = keeps[h] * n_ref[:, h, :] + key
        newn_ref[:, h, :] = new_n
        denom = jnp.maximum(
            jnp.abs(jnp.sum(new_n * query, axis=1, keepdims=True)), jnp.exp(-new_ms[h])
        )
        value = proj_rs[2 + 2 * h].total() * scale
        numer = keeps[h] * reads[h] + value * jnp.sum(key * query, axis=1, keepdims=True)
        cols_v[h] = value.T
        out_pre = proj_rs[3 + 2 * h].total() * scale
        gated = numer / ((1.0 + jnp.exp(-out_pre)) * denom)
        head_ag[h].buf[kv] = gated.astype(BF16)
        head_ag[h].send()
    for h in range(heads):
        keep_wide = jnp.broadcast_to(keeps[h], (rows, query_size))
        for b in range(rows):
            newc_ref[b, h] = (
                keep_wide[b : b + 1, :] * newc_ref[b, h] + cols_v[h, :, b : b + 1] * keys[h][b : b + 1, :]
            )
    for ag in head_ag:
        ag.relay()

    late[0].wait()
    attn = None
    for h in range(heads):
        head_ag[h].wait()
        block = head_ag[h].buf[...].astype(F32).reshape(batch, value_size).astype(BF16)
        one = jnp.dot(block, wout_v[h * value_size : (h + 1) * value_size, :], preferred_element_type=F32)
        attn = one if attn is None else attn + one
    abuf[tp] = attn.astype(BF16)
    tp_send(abuf, asem)
    for group in [gates_rs, *proj_rs, *head_ag]:
        group.settle()
    proj_queue.finish()
    proj_rs[-1].drain()
    attn_mix = tp_total(abuf, asem)
    middle = (tok_v[...].astype(F32) + attn_mix).astype(BF16)
    mid_v[...] = middle
    mid = middle.astype(F32)
    squares = jnp.sum(mid * mid, axis=1, keepdims=True)
    normed = (mid * gain2_ref[...]).astype(BF16)
    square_rs.put(jnp.broadcast_to(squares, (batch, LANES)), 0, LANES)
    late[1].wait()
    late[2].wait()
    ffn_queue = Queue([square_rs, *[rs for rs in ffn_rs if rs.inner_first]], turn.at[1], FFN_WINDOW, FFN_HAND)
    scale2 = None
    order = ffn_order(spans)
    seconds = [k for kind, k in order if kind == 1]
    for kind, k in order:
        at, wide, inner_first = spans[k]
        half = padded(wide)
        if kind == 0:
            for j, weight in enumerate([wgf_v, wuf_v]):
                out = lax.dot_general(
                    normed, weight[at : at + wide, :], (((1,), (1,)), ((), ())), preferred_element_type=F32
                )
                ffn_rs[k].put(out, j * half, wide)
                if half > wide:
                    fill = jnp.zeros((batch, half - wide), F32)
                    ffn_rs[k].put(fill, j * half + wide, half - wide)
            if k == 0:
                ffn_queue.early(0)
            if inner_first:
                ffn_queue.early(ffn_queue.scatters.index(ffn_rs[k]))
            else:
                ffn_rs[k].start()
            if k == len(spans) - 1:
                ffn_queue.late()
        elif kind == 1:
            ffn_rs[k].second()
            if k == seconds[0]:
                square_rs.second()
        elif kind == 2:
            if scale2 is None:
                total = square_rs.total()
                scale2 = lax.rsqrt(total[:, :1] / (width * count) + norm_floor)
            both = ffn_rs[k].total() * scale2
            gate = both[:, :wide]
            up = both[:, half : half + wide]
            hid = gate / (1.0 + jnp.exp(-gate)) * up
            ffn_ag[k].buf[kv] = hid.astype(BF16)
            ffn_ag[k].send()
        elif kind == 3:
            ffn_ag[k].relay()
        else:
            ffn_ag[k].wait()
            if k == 0:
                late[3].wait()
            hid = ffn_ag[k].buf[...].astype(F32).reshape(batch, wide).astype(BF16)
            one = jnp.dot(hid, wdf_v[at : at + wide, :], preferred_element_type=F32)
            if k == 0:
                acc_v[...] = one
            else:
                acc_v[...] += one
    dbuf[tp] = acc_v[...].astype(BF16)
    tp_send(dbuf, dsem)
    for group in [square_rs, *ffn_rs, *ffn_ag]:
        group.settle()
    ffn_queue.finish()
    for rs in ffn_rs:
        if not rs.inner_first:
            rs.drain()
    tp_settle(abuf, asem)
    down = tp_total(dbuf, dsem)
    mixed_ref[...] = (mid_v[...].astype(F32) + down).astype(BF16)
    tp_settle(dbuf, dsem)


def store_kernel(mixed_in, c_in, n_in, m_in, mixed_out, c_out, n_out, m_out, sems):
    rows = c_in.shape[0]
    copies = [pltpu.make_async_copy(c_in.at[b], c_out.at[b], sems.at[b]) for b in range(rows)]
    copies += [
        pltpu.make_async_copy(src, dst, sems.at[rows + i])
        for i, (src, dst) in enumerate([(mixed_in, mixed_out), (n_in, n_out), (m_in, m_out)])
    ]
    for copy in copies:
        copy.start()
    for copy in copies:
        copy.wait()


def per_device(
    tokens,
    attn_gain,
    w_query,
    w_key,
    w_value,
    w_outgate,
    w_gates,
    forget_bias,
    state_c,
    state_n,
    state_m,
    w_output,
    mlp_gain,
    w_gateff,
    w_upff,
    w_downff,
):
    count = lax.axis_size("kv")
    tps = lax.axis_size("tp")
    batch, width = tokens.shape
    rows, heads, value_size, query_size = state_c.shape
    hidden = w_gateff.shape[1]
    inner = inner_size(count)
    outer = count // inner
    spans = hidden_spans(hidden)
    sem = pltpu.SemaphoreType.DMA
    struct = jax.ShapeDtypeStruct
    args = (
        tokens, attn_gain[None], w_query, w_key, w_value, w_outgate, w_gates.T,
        forget_bias[None], state_m.T, state_n, state_c, w_output, mlp_gain[None],
        w_gateff.T, w_upff.T, w_downff,
    )
    chunks = [heads * query_size] * 2 + [value_size] * (2 * heads)
    scratch = [
        pltpu.VMEM(tokens.shape, BF16),
        pltpu.VMEM((1, width), F32),
        *[pltpu.VMEM(w.shape, BF16) for w in (w_query, w_key, w_value, w_outgate)],
        pltpu.VMEM((w_gates.shape[1], width), BF16),
        *[pltpu.VMEM(w.shape, BF16) for w in (w_output, w_gateff.T, w_upff.T, w_downff)],
        *[pltpu.VMEM(args[i].shape, F32) for i in (7, 8, 9, 12)],
        pltpu.VMEM(state_c.shape, BF16),
        sem((7 + len(chunks),)),
        sem,
        sem((4,)),
    ]
    scratch += scatter_scratch(inner, outer, rows, LANES, F32)
    for wide in chunks[:-1]:
        scratch += scatter_scratch(inner, outer, rows, wide, BF16)
    scratch += scatter_scratch(outer, inner, rows, chunks[-1], BF16)
    for _ in range(heads):
        scratch += gather_scratch(count, rows, value_size)
    for _, wide, inner_first in spans:
        firsts, seconds = (inner, outer) if inner_first else (outer, inner)
        scratch += scatter_scratch(firsts, seconds, rows, 2 * padded(wide), BF16)
    scratch += scatter_scratch(inner, outer, rows, LANES, F32)
    for _, wide, _ in spans:
        scratch += gather_scratch(count, rows, wide)
    scratch += [
        pltpu.VMEM((tps, batch, width), BF16),
        pltpu.VMEM((tps, batch, width), BF16),
        pltpu.VMEM((batch, width), BF16),
        pltpu.VMEM((batch, width), F32),
        pltpu.VMEM((heads, value_size, rows), F32),
        *[sem((2,))] * 2,
        pltpu.SemaphoreType.REGULAR((2,)),
    ]

    def kernel(*refs):
        layer_kernel(heads, spans, *refs)

    kernel_outs = (
        struct((batch, width), BF16),
        struct(state_c.shape, F32),
        struct(state_n.shape, F32),
        struct(state_m.T.shape, F32),
    )
    state_bytes = state_c.size * 4
    outs = pl.pallas_call(
        kernel,
        out_shape=kernel_outs,
        in_specs=[HBM_SPEC] * len(args),
        out_specs=(VMEM_SPEC,) * 4,
        scratch_shapes=scratch,
        compiler_params=pltpu.CompilerParams(
            collective_id=0, has_side_effects=True,
            vmem_limit_bytes=VMEM_ALL - 3 * state_bytes,
        ),
        name="layer",
    )(*[pltpu.with_memory_space_constraint(arg, pltpu.HBM) for arg in args])
    mixed, new_c, new_n, new_m = pl.pallas_call(
        store_kernel,
        out_shape=kernel_outs,
        in_specs=[VMEM_SPEC] * 4,
        out_specs=(HBM_SPEC,) * 4,
        scratch_shapes=[sem((rows + 3,))],
        compiler_params=pltpu.CompilerParams(vmem_limit_bytes=ROOM),
        name="store",
    )(*outs)
    return (mixed, new_c, new_n, new_m.T)


def solution(mesh):
    placed = (
        P(None, "kv"),
        P("kv"),
        P("kv", "tp"),
        P("kv", "tp"),
        P("kv", "tp"),
        P("kv", "tp"),
        P(),
        P(),
        P("kv", "tp", None, None),
        P("kv", "tp", None),
        P("kv", "tp"),
        P("tp", "kv"),
        P("kv"),
        P("kv", "tp"),
        P("kv", "tp"),
        P("tp", "kv"),
    )
    return jax.shard_map(
        per_device,
        mesh=mesh,
        in_specs=placed,
        out_specs=(P(None, "kv"), P("kv", "tp", None, None), P("kv", "tp", None), P("kv", "tp")),
        check_vma=False,
    )
```
